512 devices in a mesh: sp: 64 (over z, y), tp: 8 (over x, core).
Axes of the slice: x: 4, y: 4, z: 16, core: 2. Of those that a mesh axis runs over, the one named last changes fastest.
Arguments:
- queries: bfloat16 [32768, 1024], P('sp', 'tp'), may hold values from -8 to 8
- key_rows: bfloat16 [32768, 512], P('sp', 'tp'), may hold values from -8 to 8
- values: bfloat16 [32768, 512], P('sp', 'tp'), may hold values from -16 to 16
- doc_ids: int32 [32768], P('sp'), may hold values from 0 to 31, never falling along the last dimension, each value on 1 to 2048 neighbouring positions
- sink_logits: float32 [16], P('tp'), may hold values from 2.5 to 6
- residual: bfloat16 [32768, 2048], P('sp'), may hold values from -6 to 6
- out_weight: bfloat16 [1024, 2048], P('tp'), may hold values from -0.1875 to 0.1875
- norm_gain: float32 [2048], replicated, may hold values from 0.1 to 1.9
- w_gate: bfloat16 [2048, 5632], P('sp', 'tp'), may hold values from -0.125 to 0.125
- w_up: bfloat16 [2048, 5632], P('sp', 'tp'), may hold values from -0.125 to 0.125
- w_down: bfloat16 [5632, 2048], P('tp', 'sp'), may hold values from -0.078125 to 0.078125
Outputs:
- layer_out: bfloat16 [32768, 2048], P('sp')
The draws below stay inside these ranges and needn't reach their ends.
Inputs may be any that keep to these rules, and one draw needn't show every extreme that they name: `doc_ids`: document numbers never fall along the positions; each document has 1 to 2048 positions.
All inputs are finite; a program needn't handle non-finite values.
Results may differ from the reference program's by a relative error of at most 0.014.
Values may be sent and summed in bfloat16 or wider, within the bound.
No kernel may reach another device: no remote copies, remote signals or barrier semaphores. Data moves between devices by JAX's collectives and lax.ppermute only.
A program may use at most 64 MiB of HBM per device.

```python
import math
import jax
import jax.numpy as jnp
import numpy as np
from jax import lax

D = 2048
HEADS = 16
KV_HEADS = 8
HD = 64
FF = 5632
WINDOW = 128
TOKENS = 32768
DOCS = 32
DOC_MOST = 2048
N_TP = 8


def drawn_pair(key):
    query_key = jax.random.fold_in(key, 101)
    row_key = jax.random.fold_in(key, 102)
    queries = jnp.clip(jax.random.normal(query_key, (TOKENS, HEADS * HD), jnp.float32), -6.0, 6.0)
    key_rows = jnp.clip(jax.random.normal(row_key, (TOKENS, KV_HEADS * HD), jnp.float32), -6.0, 6.0)
    return (queries, key_rows)


def draw_queries(key, part):
    return drawn_pair(key)[0].astype(jnp.bfloat16)


def draw_key_rows(key, part):
    return drawn_pair(key)[1].astype(jnp.bfloat16)


def steps_of(stream_key, dims, split, low, high):
    loudness, own = 1.0, jax.random.fold_in(stream_key, 6)
    for position, shards_of in split:
        steps = jnp.exp(jax.random.uniform(jax.random.fold_in(own, position), (shards_of,), jnp.float32, low / len(split), high / len(split)))
        loudness = loudness * jnp.repeat(steps, dims[position] // shards_of).reshape([-1 if axis == position else 1 for axis in range(len(dims))])
    return loudness


def split_up(number_of, total, most, skew):
    loads = [(1 << 20) // math.isqrt(grade ** skew) + 1 for grade in range(2, number_of + 1)]
    rest, given = total - most - (number_of - 1), [1] * (number_of - 1)
    while rest > 0:
        candidates = [i for i in range(number_of - 1) if given[i] < most]
        pool, remaining = sum([loads[i] for i in candidates]), rest
        for i in candidates:
            more = min(most - given[i], max(1, remaining * loads[i] // pool), rest)
            given[i] = given[i] + more
            rest = rest - more
    return np.array([most] + given)


def uneven_parts(stream_key, amount, total, reach, slope):
    if amount == 2:
        one = jax.random.randint(stream_key, (), max(1, total - reach), min(reach, total - 1) + 1)
        return jnp.stack([one, total - one])
    lengths = jnp.asarray(split_up(amount, total, reach, slope), jnp.int32)
    couples = (amount - 1) // 2
    source_of, taker = lengths[1:1 + 2 * couples:2], lengths[2:2 + 2 * couples:2]
    room = jnp.minimum(source_of - 1, reach - taker)
    moved = jax.random.randint(jax.random.fold_in(stream_key, 1), (couples,), 0, 1 << 20) % (room + 1)
    lengths = lengths.at[1:1 + 2 * couples:2].set(source_of - moved).at[2:2 + 2 * couples:2].set(taker + moved)
    return lengths[jax.random.permutation(jax.random.fold_in(stream_key, 2), amount)]


def scatter_about(own_key, extent, width, limit, cuts=(), kind=jnp.bfloat16):
    entries = width * jax.random.normal(own_key, extent, jnp.float32)
    if cuts:
        entries = entries * steps_of(own_key, extent, cuts, -0.22, 0.18)
    return jnp.clip(entries, -limit, limit).astype(kind)


def setup_inputs(seed: int = 0) -> dict:
    seeds = jax.random.split(jax.random.key(seed), 12)
    return {
        "queries": draw_queries(jax.random.fold_in(seeds[11], 71), 0),
        "key_rows": draw_key_rows(jax.random.fold_in(seeds[11], 71), 0),
        "values": scatter_about(seeds[2], (TOKENS, KV_HEADS * HD), 3.0, 16.0, ((0, 64), (1, 8))),
        "doc_ids": jnp.searchsorted(jnp.cumsum(uneven_parts(seeds[3], DOCS, TOKENS, DOC_MOST, 1)), jnp.arange(TOKENS), side="right").astype(jnp.int32),
        "sink_logits": jnp.clip(2.5 + 3.5 * jax.random.uniform(seeds[4], (HEADS,), jnp.float32) ** steps_of(seeds[4], (HEADS,), ((0, 8),), -0.2, 0.2), 2.5, 6.0),
        "residual": scatter_about(seeds[5], (TOKENS, D), 1.0, 6.0, ((0, 64),)),
        "out_weight": scatter_about(seeds[6], (HEADS * HD, D), (HEADS * HD) ** -0.5, 0.1875, ((0, 8),)),
        "norm_gain": jnp.clip(1.0 + 0.18 * jax.random.normal(seeds[7], (D,), jnp.float32), 0.1, 1.9),
        "w_gate": scatter_about(seeds[8], (D, FF), D ** -0.5, 0.125, ((0, 64), (1, 8))),
        "w_up": scatter_about(seeds[9], (D, FF), D ** -0.5, 0.125, ((0, 64), (1, 8))),
        "w_down": scatter_about(seeds[10], (FF, D), FF ** -0.5, 0.078125, ((0, 8), (1, 64))),
    }


def rms_norm(stream, norm_gain):
    floats = stream.astype(jnp.float32)
    scale = lax.rsqrt(lax.optimization_barrier(jnp.mean(floats * floats, axis=-1, keepdims=True)) + 1e-06)
    return floats * scale * norm_gain

def band_rows(tensor, blocks):
    tensor = tensor.reshape((blocks + 1, WINDOW) + tensor.shape[1:])
    return jnp.concatenate([tensor[:-1], tensor[1:]], axis=1)

def sliding(queries, key_rows, values, doc_ids, sink_logits):
    total_rows = queries.shape[0]
    blocks = total_rows // WINDOW
    per_kv = HEADS // KV_HEADS
    pad_rows = jnp.zeros((WINDOW, KV_HEADS * HD), jnp.bfloat16)
    key_band = band_rows(jnp.concatenate([pad_rows, key_rows], axis=0), blocks)
    value_band = band_rows(jnp.concatenate([pad_rows, values], axis=0), blocks)
    doc_band = band_rows(jnp.concatenate([jnp.full((WINDOW,), -1, jnp.int32), doc_ids.astype(jnp.int32)]), blocks)
    key_band = key_band.reshape(blocks, 2 * WINDOW, KV_HEADS, HD).astype(jnp.float32)
    value_band = value_band.reshape(blocks, 2 * WINDOW, KV_HEADS, HD).astype(jnp.float32)
    query_band = queries.reshape(blocks, WINDOW, KV_HEADS, per_kv, HD).astype(jnp.float32)
    scores = jnp.einsum('nqhgd,nkhd->nhgqk', query_band, key_band) * HD ** (-0.5)
    offsets = jnp.arange(WINDOW)[:, None] + WINDOW - jnp.arange(2 * WINDOW)[None, :]
    inside = (offsets >= 0) & (offsets < WINDOW)
    query_docs = doc_ids.reshape(blocks, WINDOW)
    allowed = inside[None] & (query_docs[:, :, None] == doc_band[:, None, :])
    scores = jnp.where(allowed[:, None, None], scores, -1e+30)
    sink_logit = sink_logits.reshape(KV_HEADS, per_kv)[None, :, :, None, None]
    peak = jnp.maximum(lax.optimization_barrier(jnp.max(scores, axis=-1, keepdims=True)), sink_logit)
    raised = jnp.exp(scores - peak)
    denom = lax.optimization_barrier(jnp.sum(raised, axis=-1, keepdims=True)) + jnp.exp(sink_logit - peak)
    weights = (raised / denom).astype(jnp.bfloat16)
    attended = jnp.einsum('nhgqk,nkhd->nqhgd', weights.astype(jnp.float32), value_band)
    return attended.astype(jnp.bfloat16).reshape(total_rows, HEADS * HD)

def grouped_sum(left, right, parts):
    columns = left.shape[1] // parts

    def one(carry, index):
        piece = lax.dynamic_slice_in_dim(left, (index * columns).astype(jnp.int32), columns, 1)
        weight = lax.dynamic_slice_in_dim(right, (index * columns).astype(jnp.int32), columns, 0)
        partial_term = jnp.dot(piece, weight, preferred_element_type=jnp.float32).astype(jnp.bfloat16)
        partial_term = lax.optimization_barrier(partial_term)
        return (carry + partial_term.astype(jnp.float32), None)
    start_acc = jnp.zeros((left.shape[0], right.shape[1]), jnp.float32)
    summed, _ = lax.scan(one, start_acc, jnp.arange(parts, dtype=jnp.int32))
    return summed

def feed_forward(normed, w_gate, w_up, w_down, parts):
    columns = w_gate.shape[1] // parts

    def one(carry, index):
        offset = (index * columns).astype(jnp.int32)
        gate_act = jnp.dot(normed, lax.dynamic_slice_in_dim(w_gate, offset, columns, 1), preferred_element_type=jnp.float32)
        up_act = jnp.dot(normed, lax.dynamic_slice_in_dim(w_up, offset, columns, 1), preferred_element_type=jnp.float32)
        hidden = (jax.nn.silu(gate_act) * up_act).astype(jnp.bfloat16)
        weight = lax.dynamic_slice_in_dim(w_down, offset, columns, 0)
        partial_term = jnp.dot(hidden, weight, preferred_element_type=jnp.float32).astype(jnp.bfloat16)
        partial_term = lax.optimization_barrier(partial_term)
        return (carry + partial_term.astype(jnp.float32), None)
    start_acc = jnp.zeros((normed.shape[0], w_down.shape[1]), jnp.float32)
    summed, _ = lax.scan(one, start_acc, jnp.arange(parts, dtype=jnp.int32))
    return summed

def reference(queries, key_rows, values, doc_ids, sink_logits, residual, out_weight, norm_gain, w_gate, w_up, w_down):
    attended = sliding(queries, key_rows, values, doc_ids, sink_logits)
    mixed_sum = grouped_sum(attended, out_weight, N_TP)
    stream = (residual.astype(jnp.float32) + mixed_sum).astype(jnp.bfloat16)
    normed = rms_norm(stream, norm_gain).astype(jnp.bfloat16)
    mlp_total = feed_forward(normed, w_gate, w_up, w_down, N_TP)
    return (stream.astype(jnp.float32) + mlp_total).astype(jnp.bfloat16)
```

```python
import jax
import jax.numpy as jnp
from jax import lax
from jax.sharding import PartitionSpec as P

HD = 64
WINDOW = 128
NZ, NY, NX = 16, 4, 4
FAR_Z = [[z * NY + y for z in range(NZ)] for y in range(NY)]
FAR_Y = [[z * NY + y for y in range(NY)] for z in range(NZ)]
FAR_X = [[2 * x + c for x in range(NX)] for c in range(2)]


def from_behind(shard, axis, by):
    size = lax.axis_size(axis)
    pairs = [(i, i + by) for i in range(size) if 0 <= i + by < size]
    return lax.ppermute(shard, axis, pairs)


def other_core(shard):
    return lax.ppermute(shard, "tp", [(i, i ^ 1) for i in range(2 * NX)])


def swapped(pieces, axis, groups):
    return lax.all_to_all(pieces, axis, 0, 0, tiled=True, axis_index_groups=groups)


def copies(shard, axis, groups):
    return swapped(jnp.broadcast_to(shard[None], (len(groups[0]), *shard.shape)), axis, groups)


def rms_norm(stream, norm_gain):
    floats = stream.astype(jnp.float32)
    scale = lax.rsqrt(jnp.mean(floats * floats, axis=-1, keepdims=True) + 1e-06)
    return floats * scale * norm_gain


def band_rows(tensor, blocks):
    tensor = tensor.reshape((blocks + 1, WINDOW) + tensor.shape[1:])
    return jnp.concatenate([tensor[:-1], tensor[1:]], axis=1)


def attend(queries, key_rows, values, doc_ids, sink_logits):
    local_rows = queries.shape[0]
    blocks = local_rows // WINDOW
    kv_local = key_rows.shape[1] // HD
    per_kv = queries.shape[1] // key_rows.shape[1]
    width = key_rows.shape[1]
    tail = local_rows - WINDOW
    tail_docs = (doc_ids[tail:] + 1).astype(jnp.bfloat16)
    tail_rows = jnp.concatenate([key_rows[tail:], values[tail:]], axis=1)
    docs_rows = jnp.broadcast_to(tail_docs.reshape(-1, 2 * width), (8 * WINDOW // (2 * width), 2 * width))
    before = from_behind(jnp.concatenate([tail_rows, docs_rows], axis=0), "sp", 1)
    prev_keys, prev_values = before[:WINDOW, :width], before[:WINDOW, width:]
    prev_docs = before[WINDOW].reshape(-1).astype(jnp.int32) - 1
    key_band = band_rows(jnp.concatenate([prev_keys, key_rows], axis=0), blocks).reshape(
        blocks, 2 * WINDOW, kv_local, HD
    )
    value_band = band_rows(jnp.concatenate([prev_values, values], axis=0), blocks).reshape(
        blocks, 2 * WINDOW, kv_local, HD
    )
    doc_band = band_rows(jnp.concatenate([prev_docs, doc_ids]), blocks)
    query_band = queries.reshape(blocks, WINDOW, kv_local, per_kv, HD)
    scores = jnp.einsum(
        "nqhgd,nkhd->nhgqk", query_band, key_band, preferred_element_type=jnp.float32
    ) * HD ** (-0.5)
    offsets = jnp.arange(WINDOW)[:, None] + WINDOW - jnp.arange(2 * WINDOW)[None, :]
    inside = (offsets >= 0) & (offsets < WINDOW)
    query_docs = doc_ids.reshape(blocks, WINDOW)
    allowed = inside[None] & (query_docs[:, :, None] == doc_band[:, None, :])
    scores = jnp.where(allowed[:, None, None], scores, -1e30)
    sink_logit = sink_logits.reshape(kv_local, per_kv)[None, :, :, None, None]
    peak = jnp.maximum(jnp.max(scores, axis=-1, keepdims=True), sink_logit)
    raised = jnp.exp(scores - peak)
    denom = jnp.sum(raised, axis=-1, keepdims=True) + jnp.exp(sink_logit - peak)
    weights = (raised / denom).astype(jnp.bfloat16)
    attended = jnp.einsum(
        "nhgqk,nkhd->nqhgd", weights, value_band, preferred_element_type=jnp.float32
    )
    return attended.astype(jnp.bfloat16).reshape(local_rows, queries.shape[1])


def sum_at_owner(theirs, mine):
    arrived = other_core(theirs)
    pair_sum = (mine + arrived.astype(jnp.float32)).astype(jnp.bfloat16)
    pieces = swapped(pair_sum.reshape(NX, -1, pair_sum.shape[1]), "tp", FAR_X)
    return pieces.astype(jnp.float32).sum(axis=0)


def on_device(
    queries,
    key_rows,
    values,
    doc_ids,
    sink_logits,
    residual,
    out_weight,
    norm_gain,
    w_gate,
    w_up,
    w_down,
):
    rows, width = residual.shape
    half, share = rows // 2, rows // (2 * NX)
    core = lax.rem(lax.axis_index("tp"), 2)
    chip = lax.div(lax.axis_index("tp"), 2)
    ff = w_gate.shape[1]

    near = copies(jnp.concatenate([w_gate, w_up], axis=1), "sp", FAR_Y)
    near = near.reshape(-1, 2 * ff)
    gate_up = lax.all_gather(near, "sp", axis=0, tiled=True, axis_index_groups=FAR_Z)
    column = lax.all_gather(w_down.T, "sp", axis=0, tiled=True, axis_index_groups=FAR_Z)
    down = copies(column, "sp", FAR_Y)
    down = jnp.swapaxes(down.reshape(NY, NZ, -1, ff), 0, 1).reshape(width, ff)

    attended = attend(queries, key_rows, values, doc_ids, sink_logits)
    at_mine = lax.dynamic_slice_in_dim(attended, core * half, half, 0)
    at_theirs = lax.dynamic_slice_in_dim(attended, (1 - core) * half, half, 0)
    mixed_sum = sum_at_owner(
        jnp.dot(at_theirs, out_weight, preferred_element_type=jnp.float32).astype(jnp.bfloat16),
        jnp.dot(at_mine, out_weight, preferred_element_type=jnp.float32),
    )
    base_rows = lax.dynamic_slice_in_dim(residual, core * half + chip * share, share, 0)
    stream = (base_rows.astype(jnp.float32) + mixed_sum).astype(jnp.bfloat16)
    normed = rms_norm(stream, norm_gain).astype(jnp.bfloat16)
    normed = copies(normed, "tp", FAR_X).reshape(half, width)
    normed = jnp.concatenate([normed, other_core(normed)], axis=0)

    acts = jnp.dot(normed, gate_up, preferred_element_type=jnp.float32)
    hidden = (jax.nn.silu(acts[:, :ff]) * acts[:, ff:]).astype(jnp.bfloat16)

    def through(part):
        return lax.dot_general(
            part, down, (((1,), (1,)), ((), ())), preferred_element_type=jnp.float32
        )

    mlp_total = sum_at_owner(through(hidden[half:]).astype(jnp.bfloat16), through(hidden[:half]))
    finished = (stream.astype(jnp.float32) + mlp_total).astype(jnp.bfloat16)
    mine = copies(finished, "tp", FAR_X).reshape(half, width)
    theirs = other_core(mine)
    return jnp.where(
        core == 0,
        jnp.concatenate([mine, theirs], axis=0),
        jnp.concatenate([theirs, mine], axis=0),
    )


def solution(mesh):
    in_specs = (
        P("sp", "tp"),
        P("sp", "tp"),
        P("sp", "tp"),
        P("sp"),
        P("tp"),
        P("sp", None),
        P("tp", None),
        P(),
        P("sp", "tp"),
        P("sp", "tp"),
        P("tp", "sp"),
    )
    out_specs = P("sp", None)
    return jax.shard_map(
        on_device, mesh=mesh, in_specs=in_specs, out_specs=out_specs, check_vma=False
    )
```

```python
import jax
import jax.numpy as jnp
from jax import lax
from jax.sharding import PartitionSpec as P

HD = 64
WINDOW = 128
NZ, NY, NX = 16, 4, 4
FAR_Z = [[z * NY + y for z in range(NZ)] for y in range(NY)]
FAR_Y = [[z * NY + y for y in range(NY)] for z in range(NZ)]
FAR_X = [[2 * x + c for x in range(NX)] for c in range(2)]


def from_behind(shard, axis, by):
    size = lax.axis_size(axis)
    pairs = [(i, i + by) for i in range(size) if 0 <= i + by < size]
    return lax.ppermute(shard, axis, pairs)


def other_core(shard):
    return lax.ppermute(shard, "tp", [(i, i ^ 1) for i in range(2 * NX)])


def swapped(pieces, axis, groups):
    return lax.all_to_all(pieces, axis, 0, 0, tiled=True, axis_index_groups=groups)


def copies(shard, axis, groups):
    return swapped(jnp.broadcast_to(shard[None], (len(groups[0]), *shard.shape)), axis, groups)


def chip_away(shard, by):
    pairs = [(2 * x + c, 2 * ((x + by) % NX) + c) for x in range(NX) for c in range(2)]
    return lax.ppermute(shard, "tp", pairs)


def all_chips_rows(shard, chip):
    share = shard.shape[0]
    rows = jnp.zeros((NX * share, shard.shape[1]), shard.dtype)
    rows = lax.dynamic_update_slice_in_dim(rows, shard, chip * share, 0)
    for by in (1, 3, 2):
        sender = lax.rem(chip - by + NX, NX)
        rows = lax.dynamic_update_slice_in_dim(rows, chip_away(shard, by), sender * share, 0)
    return rows


def rms_norm(stream, norm_gain):
    floats = stream.astype(jnp.float32)
    scale = lax.rsqrt(jnp.mean(floats * floats, axis=-1, keepdims=True) + 1e-06)
    return floats * scale * norm_gain


def band_rows(tensor, blocks):
    tensor = tensor.reshape((blocks + 1, WINDOW) + tensor.shape[1:])
    return jnp.concatenate([tensor[:-1], tensor[1:]], axis=1)


def attend(queries, key_rows, values, doc_ids, sink_logits):
    local_rows = queries.shape[0]
    blocks = local_rows // WINDOW
    kv_local = key_rows.shape[1] // HD
    per_kv = queries.shape[1] // key_rows.shape[1]
    width = key_rows.shape[1]
    tail = local_rows - WINDOW
    tail_docs = (doc_ids[tail:] + 1).astype(jnp.bfloat16)
    tail_rows = jnp.concatenate([key_rows[tail:], values[tail:]], axis=1)
    docs_rows = jnp.broadcast_to(tail_docs.reshape(-1, 2 * width), (8 * WINDOW // (2 * width), 2 * width))
    before = from_behind(jnp.concatenate([tail_rows, docs_rows], axis=0), "sp", 1)
    prev_keys, prev_values = before[:WINDOW, :width], before[:WINDOW, width:]
    prev_docs = before[WINDOW].reshape(-1).astype(jnp.int32) - 1
    key_band = band_rows(jnp.concatenate([prev_keys, key_rows], axis=0), blocks).reshape(
        blocks, 2 * WINDOW, kv_local, HD
    )
    value_band = band_rows(jnp.concatenate([prev_values, values], axis=0), blocks).reshape(
        blocks, 2 * WINDOW, kv_local, HD
    )
    doc_band = band_rows(jnp.concatenate([prev_docs, doc_ids]), blocks)
    query_band = queries.reshape(blocks, WINDOW, kv_local, per_kv, HD)
    scores = jnp.einsum(
        "nqhgd,nkhd->nhgqk", query_band, key_band, preferred_element_type=jnp.float32
    ) * HD ** (-0.5)
    offsets = jnp.arange(WINDOW)[:, None] + WINDOW - jnp.arange(2 * WINDOW)[None, :]
    inside = (offsets >= 0) & (offsets < WINDOW)
    query_docs = doc_ids.reshape(blocks, WINDOW)
    allowed = inside[None] & (query_docs[:, :, None] == doc_band[:, None, :])
    scores = jnp.where(allowed[:, None, None], scores, -1e30)
    sink_logit = sink_logits.reshape(kv_local, per_kv)[None, :, :, None, None]
    peak = jnp.maximum(jnp.max(scores, axis=-1, keepdims=True), sink_logit)
    raised = jnp.exp(scores - peak)
    denom = jnp.sum(raised, axis=-1, keepdims=True) + jnp.exp(sink_logit - peak)
    weights = (raised / denom).astype(jnp.bfloat16)
    attended = jnp.einsum(
        "nhgqk,nkhd->nqhgd", weights, value_band, preferred_element_type=jnp.float32
    )
    return attended.astype(jnp.bfloat16).reshape(local_rows, queries.shape[1])


def pair_sum_of(theirs, mine):
    arrived = other_core(theirs)
    return (mine + arrived.astype(jnp.float32)).astype(jnp.bfloat16)


def to_owners(pair_sum):
    return swapped(pair_sum.reshape(NX, -1, pair_sum.shape[1]), "tp", FAR_X)


def on_device(
    queries,
    key_rows,
    values,
    doc_ids,
    sink_logits,
    residual,
    out_weight,
    norm_gain,
    w_gate,
    w_up,
    w_down,
):
    rows, width = residual.shape
    half, share = rows // 2, rows // (2 * NX)
    core = lax.rem(lax.axis_index("tp"), 2)
    chip = lax.div(lax.axis_index("tp"), 2)
    ff = w_gate.shape[1]

    near = copies(jnp.concatenate([w_gate, w_up], axis=1), "sp", FAR_Y)
    near = near.reshape(-1, 2 * ff)
    gate_up = lax.all_gather(near, "sp", axis=0, tiled=True, axis_index_groups=FAR_Z)
    attended = attend(queries, key_rows, values, doc_ids, sink_logits)
    at_mine = lax.dynamic_slice_in_dim(attended, core * half, half, 0)
    at_theirs = lax.dynamic_slice_in_dim(attended, (1 - core) * half, half, 0)
    pair_sum = pair_sum_of(
        jnp.dot(at_theirs, out_weight, preferred_element_type=jnp.float32).astype(jnp.bfloat16),
        jnp.dot(at_mine, out_weight, preferred_element_type=jnp.float32),
    )
    pieces = to_owners(pair_sum)
    padded = -(-ff // 256) * 256
    turned, _ = lax.optimization_barrier((w_down.T, pair_sum))
    turned = jnp.pad(turned, ((0, 0), (0, padded - ff)))
    column = lax.all_gather(turned, "sp", axis=0, tiled=True, axis_index_groups=FAR_Z)
    column, pieces = lax.optimization_barrier((column, pieces))
    down = copies(column, "sp", FAR_Y)
    down = jnp.swapaxes(down.reshape(NY, NZ, -1, padded), 0, 1).reshape(width, padded)
    mixed_sum = pieces.astype(jnp.float32).sum(axis=0)
    base_rows = lax.dynamic_slice_in_dim(residual, core * half + chip * share, share, 0)
    stream = (base_rows.astype(jnp.float32) + mixed_sum).astype(jnp.bfloat16)
    normed = rms_norm(stream, norm_gain).astype(jnp.bfloat16)
    normed = all_chips_rows(normed, chip)
    normed = jnp.concatenate([normed, other_core(normed)], axis=0)

    acts = jnp.dot(normed, gate_up, preferred_element_type=jnp.float32)
    hidden = (jax.nn.silu(acts[:, :ff]) * acts[:, ff:]).astype(jnp.bfloat16)
    hidden = jnp.pad(hidden, ((0, 0), (0, padded - ff)))

    def through(part):
        return lax.dot_general(
            part, down, (((1,), (1,)), ((), ())), preferred_element_type=jnp.float32
        )

    pair_sum = pair_sum_of(through(hidden[half:]).astype(jnp.bfloat16), through(hidden[:half]))
    mlp_total = to_owners(pair_sum).astype(jnp.float32).sum(axis=0)
    finished = (stream.astype(jnp.float32) + mlp_total).astype(jnp.bfloat16)
    mine = copies(finished, "tp", FAR_X).reshape(half, width)
    theirs = other_core(mine)
    return jnp.where(
        core == 0,
        jnp.concatenate([mine, theirs], axis=0),
        jnp.concatenate([theirs, mine], axis=0),
    )


def solution(mesh):
    in_specs = (
        P("sp", "tp"),
        P("sp", "tp"),
        P("sp", "tp"),
        P("sp"),
        P("tp"),
        P("sp", None),
        P("tp", None),
        P(),
        P("sp", "tp"),
        P("sp", "tp"),
        P("tp", "sp"),
    )
    out_specs = P("sp", None)
    return jax.shard_map(
        on_device, mesh=mesh, in_specs=in_specs, out_specs=out_specs, check_vma=False
    )
```

```python
import jax
import jax.numpy as jnp
from jax import lax
from jax.sharding import PartitionSpec as P


HD = 64
WINDOW = 128
NZ, NY, NX = 16, 4, 4
EARLY = 512
FAR_Z = [[z * NY + y for z in range(NZ)] for y in range(NY)]
FAR_Y = [[z * NY + y for y in range(NY)] for z in range(NZ)]
FAR_X = [[2 * x + c for x in range(NX)] for c in range(2)]


def from_behind(shard, axis, by):
    size = lax.axis_size(axis)
    pairs = [(i, i + by) for i in range(size) if 0 <= i + by < size]
    return lax.ppermute(shard, axis, pairs)


def other_core(shard):
    return lax.ppermute(shard, "tp", [(i, i ^ 1) for i in range(2 * NX)])


def swapped(pieces, axis, groups):
    return lax.all_to_all(pieces, axis, 0, 0, tiled=True, axis_index_groups=groups)


def copies(shard, axis, groups):
    return swapped(jnp.broadcast_to(shard[None], (len(groups[0]), *shard.shape)), axis, groups)


def chip_away(shard, by):
    pairs = [(2 * x + c, 2 * ((x + by) % NX) + c) for x in range(NX) for c in range(2)]
    return lax.ppermute(shard, "tp", pairs)


def all_chips_rows(shard, chip):
    share = shard.shape[0]
    rows = jnp.zeros((NX * share, shard.shape[1]), shard.dtype)
    rows = lax.dynamic_update_slice_in_dim(rows, shard, chip * share, 0)
    for by in (1, 3, 2):
        sender = lax.rem(chip - by + NX, NX)
        rows = lax.dynamic_update_slice_in_dim(rows, chip_away(shard, by), sender * share, 0)
    return rows


def rms_norm(stream, norm_gain):
    floats = stream.astype(jnp.float32)
    scale = lax.rsqrt(jnp.mean(floats * floats, axis=-1, keepdims=True) + 1e-06)
    return floats * scale * norm_gain


def band_rows(tensor, blocks):
    tensor = tensor.reshape((blocks + 1, WINDOW) + tensor.shape[1:])
    return jnp.concatenate([tensor[:-1], tensor[1:]], axis=1)


def attend(queries, key_rows, values, doc_ids, sink_logits):
    local_rows = queries.shape[0]
    blocks = local_rows // WINDOW
    kv_local = key_rows.shape[1] // HD
    per_kv = queries.shape[1] // key_rows.shape[1]
    width = key_rows.shape[1]
    tail = local_rows - WINDOW
    tail_docs = (doc_ids[tail:] + 1).astype(jnp.bfloat16)
    tail_rows = jnp.concatenate([key_rows[tail:], values[tail:]], axis=1)
    docs_rows = jnp.broadcast_to(tail_docs.reshape(-1, 2 * width), (8 * WINDOW // (2 * width), 2 * width))
    before = from_behind(jnp.concatenate([tail_rows, docs_rows], axis=0), "sp", 1)
    prev_keys, prev_values = before[:WINDOW, :width], before[:WINDOW, width:]
    prev_docs = before[WINDOW].reshape(-1).astype(jnp.int32) - 1
    key_band = band_rows(jnp.concatenate([prev_keys, key_rows], axis=0), blocks).reshape(
        blocks, 2 * WINDOW, kv_local, HD
    )
    value_band = band_rows(jnp.concatenate([prev_values, values], axis=0), blocks).reshape(
        blocks, 2 * WINDOW, kv_local, HD
    )
    doc_band = band_rows(jnp.concatenate([prev_docs, doc_ids]), blocks)
    query_band = queries.reshape(blocks, WINDOW, kv_local, per_kv, HD)
    scores = jnp.einsum(
        "nqhgd,nkhd->nhgqk", query_band, key_band, preferred_element_type=jnp.float32
    ) * HD ** (-0.5)
    offsets = jnp.arange(WINDOW)[:, None] + WINDOW - jnp.arange(2 * WINDOW)[None, :]
    inside = (offsets >= 0) & (offsets < WINDOW)
    query_docs = doc_ids.reshape(blocks, WINDOW)
    allowed = inside[None] & (query_docs[:, :, None] == doc_band[:, None, :])
    scores = jnp.where(allowed[:, None, None], scores, -1e30)
    sink_logit = sink_logits.reshape(kv_local, per_kv)[None, :, :, None, None]
    peak = jnp.maximum(jnp.max(scores, axis=-1, keepdims=True), sink_logit)
    raised = jnp.exp(scores - peak)
    denom = jnp.sum(raised, axis=-1, keepdims=True) + jnp.exp(sink_logit - peak)
    weights = (raised / denom).astype(jnp.bfloat16)
    attended = jnp.einsum(
        "nhgqk,nkhd->nqhgd", weights, value_band, preferred_element_type=jnp.float32
    )
    return attended.astype(jnp.bfloat16).reshape(local_rows, queries.shape[1])


def pair_sum_of(theirs, mine):
    arrived = other_core(theirs)
    return (mine + arrived.astype(jnp.float32)).astype(jnp.bfloat16)


def to_owners(pair_sum):
    return swapped(pair_sum.reshape(NX, -1, pair_sum.shape[1]), "tp", FAR_X)


def on_device(
    queries,
    key_rows,
    values,
    doc_ids,
    sink_logits,
    residual,
    out_weight,
    norm_gain,
    w_gate,
    w_up,
    w_down,
):
    rows, width = residual.shape
    half, share = rows // 2, rows // (2 * NX)
    core = lax.rem(lax.axis_index("tp"), 2)
    chip = lax.div(lax.axis_index("tp"), 2)
    ff = w_gate.shape[1]

    turned = w_down.T
    near = copies(jnp.concatenate([w_gate, w_up, turned[:, EARLY:]], axis=1), "sp", FAR_Y)
    near = near.reshape(-1, near.shape[2])
    far = lax.all_gather(near, "sp", axis=0, tiled=True, axis_index_groups=FAR_Z)

    attended = attend(queries, key_rows, values, doc_ids, sink_logits)
    at_mine = lax.dynamic_slice_in_dim(attended, core * half, half, 0)
    at_theirs = lax.dynamic_slice_in_dim(attended, (1 - core) * half, half, 0)
    pair_sum = pair_sum_of(
        jnp.dot(at_theirs, out_weight, preferred_element_type=jnp.float32).astype(jnp.bfloat16),
        jnp.dot(at_mine, out_weight, preferred_element_type=jnp.float32),
    )
    pieces = to_owners(pair_sum)
    early, _ = lax.optimization_barrier((turned[:, :EARLY], pair_sum))
    column = lax.all_gather(early, "sp", axis=0, tiled=True, axis_index_groups=FAR_Z)
    spread = jnp.broadcast_to(column[None], (NY, *column.shape))
    spread, pieces = lax.optimization_barrier((spread, pieces))
    down = swapped(spread, "sp", FAR_Y)
    down = jnp.swapaxes(down.reshape(NY, NZ, -1, EARLY), 0, 1).reshape(width, EARLY)
    mixed_sum = pieces.astype(jnp.float32).sum(axis=0)
    base_rows = lax.dynamic_slice_in_dim(residual, core * half + chip * share, share, 0)
    stream = (base_rows.astype(jnp.float32) + mixed_sum).astype(jnp.bfloat16)
    normed = rms_norm(stream, norm_gain).astype(jnp.bfloat16)
    normed = all_chips_rows(normed, chip)
    normed = jnp.concatenate([normed, other_core(normed)], axis=0)

    acts = jnp.dot(normed, far[:, : 2 * ff], preferred_element_type=jnp.float32)
    hidden = (jax.nn.silu(acts[:, :ff]) * acts[:, ff:]).astype(jnp.bfloat16)

    def turned_dot(left, right):
        return lax.dot_general(
            left, right, (((1,), (1,)), ((), ())), preferred_element_type=jnp.float32
        )

    late = far[:, 2 * ff :]

    def through(part):
        return turned_dot(part[:, EARLY:], late) + turned_dot(part[:, :EARLY], down)

    pair_sum = pair_sum_of(through(hidden[half:]).astype(jnp.bfloat16), through(hidden[:half]))
    mlp_total = to_owners(pair_sum).astype(jnp.float32).sum(axis=0)
    finished = (stream.astype(jnp.float32) + mlp_total).astype(jnp.bfloat16)
    mine = copies(finished, "tp", FAR_X).reshape(half, width)
    theirs = other_core(mine)
    whole = jnp.zeros((rows, width), jnp.bfloat16)
    whole = lax.dynamic_update_slice_in_dim(whole, mine, core * half, 0)
    return lax.dynamic_update_slice_in_dim(whole, theirs, (1 - core) * half, 0)


def solution(mesh):
    in_specs = (
        P("sp", "tp"),
        P("sp", "tp"),
        P("sp", "tp"),
        P("sp"),
        P("tp"),
        P("sp", None),
        P("tp", None),
        P(),
        P("sp", "tp"),
        P("sp", "tp"),
        P("tp", "sp"),
    )
    out_specs = P("sp", None)
    return jax.shard_map(
        on_device, mesh=mesh, in_specs=in_specs, out_specs=out_specs, check_vma=False
    )
```

```python
import jax
import jax.numpy as jnp
from jax import lax
from jax.sharding import PartitionSpec as P


HD = 64
WINDOW = 128
NZ, NY, NX = 16, 4, 4
EARLY = 512
FAR_Z = [[z * NY + y for z in range(NZ)] for y in range(NY)]
FAR_Y = [[z * NY + y for y in range(NY)] for z in range(NZ)]
FAR_X = [[2 * x + c for x in range(NX)] for c in range(2)]


def from_behind(shard, axis, by):
    size = lax.axis_size(axis)
    pairs = [(i, i + by) for i in range(size) if 0 <= i + by < size]
    return lax.ppermute(shard, axis, pairs)


def other_core(shard):
    return lax.ppermute(shard, "tp", [(i, i ^ 1) for i in range(2 * NX)])


def swapped(pieces, axis, groups):
    return lax.all_to_all(pieces, axis, 0, 0, tiled=True, axis_index_groups=groups)


def copies(shard, axis, groups):
    return swapped(jnp.broadcast_to(shard[None], (len(groups[0]), *shard.shape)), axis, groups)


def chip_away(shard, by):
    pairs = [(2 * x + c, 2 * ((x + by) % NX) + c) for x in range(NX) for c in range(2)]
    return lax.ppermute(shard, "tp", pairs)


def from_chips(shard):
    arrived = {by: chip_away(shard, by) for by in (2, 1, 3)}
    return [shard] + [arrived[by] for by in (1, 2, 3)]


def summed_at_owners(blocks):
    arrived = {by: chip_away(blocks[-by], by) for by in (2, 1, 3)}
    total = blocks[0].astype(jnp.float32)
    for by in (1, 3, 2):
        total = total + arrived[by].astype(jnp.float32)
    return total


def rms_norm(stream, norm_gain):
    floats = stream.astype(jnp.float32)
    scale = lax.rsqrt(jnp.mean(floats * floats, axis=-1, keepdims=True) + 1e-06)
    return floats * scale * norm_gain


def band_rows(tensor, blocks):
    tensor = tensor.reshape((blocks + 1, WINDOW) + tensor.shape[1:])
    return jnp.concatenate([tensor[:-1], tensor[1:]], axis=1)


def attend(queries, key_rows, values, doc_ids, sink_logits):
    local_rows = queries.shape[0]
    blocks = local_rows // WINDOW
    kv_local = key_rows.shape[1] // HD
    per_kv = queries.shape[1] // key_rows.shape[1]
    width = key_rows.shape[1]
    tail = local_rows - WINDOW
    tail_docs = (doc_ids[tail:] + 1).astype(jnp.bfloat16)
    tail_rows = jnp.concatenate([key_rows[tail:], values[tail:]], axis=1)
    docs_rows = jnp.broadcast_to(tail_docs.reshape(-1, 2 * width), (8 * WINDOW // (2 * width), 2 * width))
    before = from_behind(jnp.concatenate([tail_rows, docs_rows], axis=0), "sp", 1)
    prev_keys, prev_values = before[:WINDOW, :width], before[:WINDOW, width:]
    prev_docs = before[WINDOW].reshape(-1).astype(jnp.int32) - 1
    key_band = band_rows(jnp.concatenate([prev_keys, key_rows], axis=0), blocks).reshape(
        blocks, 2 * WINDOW, kv_local, HD
    )
    value_band = band_rows(jnp.concatenate([prev_values, values], axis=0), blocks).reshape(
        blocks, 2 * WINDOW, kv_local, HD
    )
    doc_band = band_rows(jnp.concatenate([prev_docs, doc_ids]), blocks)
    query_band = queries.reshape(blocks, WINDOW, kv_local, per_kv, HD)
    scores = jnp.einsum(
        "nqhgd,nkhd->nhgqk", query_band, key_band, preferred_element_type=jnp.float32
    ) * HD ** (-0.5)
    offsets = jnp.arange(WINDOW)[:, None] + WINDOW - jnp.arange(2 * WINDOW)[None, :]
    inside = (offsets >= 0) & (offsets < WINDOW)
    query_docs = doc_ids.reshape(blocks, WINDOW)
    allowed = inside[None] & (query_docs[:, :, None] == doc_band[:, None, :])
    scores = jnp.where(allowed[:, None, None], scores, -1e30)
    sink_logit = sink_logits.reshape(kv_local, per_kv)[None, :, :, None, None]
    peak = jnp.maximum(jnp.max(scores, axis=-1, keepdims=True), sink_logit)
    raised = jnp.exp(scores - peak)
    denom = jnp.sum(raised, axis=-1, keepdims=True) + jnp.exp(sink_logit - peak)
    weights = (raised / denom).astype(jnp.bfloat16)
    attended = jnp.einsum(
        "nhgqk,nkhd->nqhgd", weights, value_band, preferred_element_type=jnp.float32
    )
    return attended.astype(jnp.bfloat16).reshape(local_rows, queries.shape[1])


def pair_sum_of(theirs, mine):
    arrived = other_core(theirs)
    return (mine + arrived.astype(jnp.float32)).astype(jnp.bfloat16)


def to_owners(pair_sum):
    return swapped(pair_sum.reshape(NX, -1, pair_sum.shape[1]), "tp", FAR_X)


def on_device(
    queries,
    key_rows,
    values,
    doc_ids,
    sink_logits,
    residual,
    out_weight,
    norm_gain,
    w_gate,
    w_up,
    w_down,
):
    rows, width = residual.shape
    half, share = rows // 2, rows // (2 * NX)
    core = lax.rem(lax.axis_index("tp"), 2)
    chip = lax.div(lax.axis_index("tp"), 2)
    ff = w_gate.shape[1]

    turned = w_down.T
    near = copies(jnp.concatenate([w_gate, w_up, turned[:, EARLY:]], axis=1), "sp", FAR_Y)
    near = near.reshape(-1, near.shape[2])
    far = lax.all_gather(near, "sp", axis=0, tiled=True, axis_index_groups=FAR_Z)

    attended = attend(queries, key_rows, values, doc_ids, sink_logits)
    at_mine = lax.dynamic_slice_in_dim(attended, core * half, half, 0)
    at_theirs = lax.dynamic_slice_in_dim(attended, (1 - core) * half, half, 0)
    pair_sum = pair_sum_of(
        jnp.dot(at_theirs, out_weight, preferred_element_type=jnp.float32).astype(jnp.bfloat16),
        jnp.dot(at_mine, out_weight, preferred_element_type=jnp.float32),
    )
    pieces = to_owners(pair_sum)
    early, _ = lax.optimization_barrier((turned[:, :EARLY], pair_sum))
    column = lax.all_gather(early, "sp", axis=0, tiled=True, axis_index_groups=FAR_Z)
    spread = jnp.broadcast_to(column[None], (NY, *column.shape))
    spread, pieces = lax.optimization_barrier((spread, pieces))
    down = swapped(spread, "sp", FAR_Y)
    down = jnp.swapaxes(down.reshape(NY, NZ, -1, EARLY), 0, 1).reshape(width, EARLY)
    mixed_sum = pieces.astype(jnp.float32).sum(axis=0)
    base_rows = lax.dynamic_slice_in_dim(residual, core * half + chip * share, share, 0)
    stream = (base_rows.astype(jnp.float32) + mixed_sum).astype(jnp.bfloat16)
    normed = rms_norm(stream, norm_gain).astype(jnp.bfloat16)
    normed = jnp.concatenate(from_chips(normed), axis=0)
    normed = jnp.concatenate([normed, other_core(normed)], axis=0)

    acts = jnp.dot(normed, far[:, : 2 * ff], preferred_element_type=jnp.float32)
    hidden = (jax.nn.silu(acts[:, :ff]) * acts[:, ff:]).astype(jnp.bfloat16)

    def turned_dot(left, right):
        return lax.dot_general(
            left, right, (((1,), (1,)), ((), ())), preferred_element_type=jnp.float32
        )

    late = far[:, 2 * ff :]

    def through(part):
        return turned_dot(part[:, EARLY:], late) + turned_dot(part[:, :EARLY], down)

    arrived = other_core(through(hidden[half:]).astype(jnp.bfloat16))
    total = through(hidden[:half])
    blocks = [slice(r * share, (r + 1) * share) for r in range(NX)]
    mlp_total = summed_at_owners(
        [(total[b] + arrived[b].astype(jnp.float32)).astype(jnp.bfloat16) for b in blocks]
    )
    finished = (stream.astype(jnp.float32) + mlp_total).astype(jnp.bfloat16)
    mine = jnp.zeros((half, width), jnp.bfloat16)
    for by, block in enumerate(from_chips(finished)):
        at = lax.rem(chip - by + NX, NX) * share
        mine = lax.dynamic_update_slice_in_dim(mine, block, at, 0)
    theirs = other_core(mine)
    whole = jnp.zeros((rows, width), jnp.bfloat16)
    whole = lax.dynamic_update_slice_in_dim(whole, mine, core * half, 0)
    return lax.dynamic_update_slice_in_dim(whole, theirs, (1 - core) * half, 0)


def solution(mesh):
    in_specs = (
        P("sp", "tp"),
        P("sp", "tp"),
        P("sp", "tp"),
        P("sp"),
        P("tp"),
        P("sp", None),
        P("tp", None),
        P(),
        P("sp", "tp"),
        P("sp", "tp"),
        P("tp", "sp"),
    )
    out_specs = P("sp", None)
    return jax.shard_map(
        on_device, mesh=mesh, in_specs=in_specs, out_specs=out_specs, check_vma=False
    )
```

```python
import jax
import jax.numpy as jnp
from jax import lax
from jax.experimental import pallas as pl
from jax.experimental.pallas import tpu as pltpu
from jax.sharding import PartitionSpec as P


HD = 64
WINDOW = 128
NZ, NY, NX = 16, 4, 4
EARLY = 640
IN_VMEM = pl.BlockSpec(memory_space=pltpu.VMEM)
IN_HBM = pl.BlockSpec(memory_space=pltpu.HBM)
FAR_Z = [[z * NY + y for z in range(NZ)] for y in range(NY)]
FAR_Y = [[z * NY + y for y in range(NY)] for z in range(NZ)]
FAR_X = [[2 * x + c for x in range(NX)] for c in range(2)]


def from_behind(shard, axis, by):
    size = lax.axis_size(axis)
    pairs = [(i, i + by) for i in range(size) if 0 <= i + by < size]
    return lax.ppermute(shard, axis, pairs)


def other_core(shard):
    return lax.ppermute(shard, "tp", [(i, i ^ 1) for i in range(2 * NX)])


def swapped(pieces, axis, groups):
    return lax.all_to_all(pieces, axis, 0, 0, tiled=True, axis_index_groups=groups)


def copies(shard, axis, groups):
    return swapped(jnp.broadcast_to(shard[None], (len(groups[0]), *shard.shape)), axis, groups)


def chip_away(shard, by):
    pairs = [(2 * x + c, 2 * ((x + by) % NX) + c) for x in range(NX) for c in range(2)]
    return lax.ppermute(shard, "tp", pairs)


def all_chips_rows(shard, chip, rows):
    share = shard.shape[0]
    rows = lax.dynamic_update_slice_in_dim(rows, shard, chip * share, 0)
    for by in (1, 3, 2):
        sender = lax.rem(chip - by + NX, NX)
        rows = lax.dynamic_update_slice_in_dim(rows, chip_away(shard, by), sender * share, 0)
    return rows


def rms_norm(stream, norm_gain):
    floats = stream.astype(jnp.float32)
    scale = lax.rsqrt(jnp.mean(floats * floats, axis=-1, keepdims=True) + 1e-06)
    return floats * scale * norm_gain


def band_rows(tensor, blocks):
    tensor = tensor.reshape((blocks + 1, WINDOW) + tensor.shape[1:])
    return jnp.concatenate([tensor[:-1], tensor[1:]], axis=1)


def attend(queries, key_rows, values, doc_ids, sink_logits):
    local_rows = queries.shape[0]
    blocks = local_rows // WINDOW
    kv_local = key_rows.shape[1] // HD
    per_kv = queries.shape[1] // key_rows.shape[1]
    width = key_rows.shape[1]
    tail = local_rows - WINDOW
    tail_docs = (doc_ids[tail:] + 1).astype(jnp.bfloat16)
    tail_rows = jnp.concatenate([key_rows[tail:], values[tail:]], axis=1)
    docs_rows = jnp.broadcast_to(tail_docs.reshape(-1, 2 * width), (8 * WINDOW // (2 * width), 2 * width))
    before = from_behind(jnp.concatenate([tail_rows, docs_rows], axis=0), "sp", 1)
    prev_keys, prev_values = before[:WINDOW, :width], before[:WINDOW, width:]
    prev_docs = before[WINDOW].reshape(-1).astype(jnp.int32) - 1
    key_band = band_rows(jnp.concatenate([prev_keys, key_rows], axis=0), blocks).reshape(
        blocks, 2 * WINDOW, kv_local, HD
    )
    value_band = band_rows(jnp.concatenate([prev_values, values], axis=0), blocks).reshape(
        blocks, 2 * WINDOW, kv_local, HD
    )
    doc_band = band_rows(jnp.concatenate([prev_docs, doc_ids]), blocks)
    query_band = queries.reshape(blocks, WINDOW, kv_local, per_kv, HD)
    scores = jnp.einsum(
        "nqhgd,nkhd->nhgqk", query_band, key_band, preferred_element_type=jnp.float32
    ) * HD ** (-0.5)
    offsets = jnp.arange(WINDOW)[:, None] + WINDOW - jnp.arange(2 * WINDOW)[None, :]
    inside = (offsets >= 0) & (offsets < WINDOW)
    query_docs = doc_ids.reshape(blocks, WINDOW)
    allowed = inside[None] & (query_docs[:, :, None] == doc_band[:, None, :])
    scores = jnp.where(allowed[:, None, None], scores, -1e30)
    sink_logit = sink_logits.reshape(kv_local, per_kv)[None, :, :, None, None]
    peak = jnp.maximum(jnp.max(scores, axis=-1, keepdims=True), sink_logit)
    raised = jnp.exp(scores - peak)
    denom = jnp.sum(raised, axis=-1, keepdims=True) + jnp.exp(sink_logit - peak)
    weights = (raised / denom).astype(jnp.bfloat16)
    attended = jnp.einsum(
        "nhgqk,nkhd->nqhgd", weights, value_band, preferred_element_type=jnp.float32
    )
    return attended.astype(jnp.bfloat16).reshape(local_rows, queries.shape[1])


def pair_sum_of(theirs, mine):
    arrived = other_core(theirs)
    return (mine + arrived.astype(jnp.float32)).astype(jnp.bfloat16)


def to_owners(pair_sum):
    return swapped(pair_sum.reshape(NX, -1, pair_sum.shape[1]), "tp", FAR_X)


def gated(mine, theirs, far, ff):
    half, width = mine.shape
    columns = far.shape[1]
    steps = 4
    depth = width // steps

    def kernel(mine_ref, theirs_ref, far_ref, hidden_ref, late_ref, rows, held, acts_ref, arrived):
        moves = []
        for k in range(steps):
            at = pl.ds(k * depth, depth)
            pairs = (
                (mine_ref.at[:, at], rows.at[k, pl.ds(0, half)]),
                (theirs_ref.at[:, at], rows.at[k, pl.ds(half, half)]),
                (far_ref.at[at], held.at[k]),
            )
            moves.append(
                [pltpu.make_async_copy(*pair, arrived.at[k, i]) for i, pair in enumerate(pairs)]
            )
        for move in moves[0] + moves[1]:
            move.start()
        for k in range(steps):
            for move in moves[k]:
                move.wait()
            if k + 2 < steps:
                for move in moves[k + 2]:
                    move.start()
            late_ref[k * depth : (k + 1) * depth, :] = held[k, :, 2 * ff :]
            part = jnp.dot(rows[k], held[k, :, : 2 * ff], preferred_element_type=jnp.float32)
            if k == 0:
                acts_ref[...] = part
            elif k < steps - 1:
                acts_ref[...] += part
            else:
                acts = acts_ref[...] + part
                hidden_ref[...] = (jax.nn.silu(acts[:, :ff]) * acts[:, ff:]).astype(jnp.bfloat16)

    return pl.pallas_call(
        kernel,
        out_shape=(
            jax.ShapeDtypeStruct((2 * half, ff), jnp.bfloat16),
            jax.ShapeDtypeStruct((width, columns - 2 * ff), jnp.bfloat16),
        ),
        in_specs=[IN_HBM] * 3,
        out_specs=(IN_VMEM, IN_VMEM),
        scratch_shapes=[
            pltpu.VMEM((steps, 2 * half, depth), jnp.bfloat16),
            pltpu.VMEM((steps, depth, columns), jnp.bfloat16),
            pltpu.VMEM((2 * half, 2 * ff), jnp.float32),
            pltpu.SemaphoreType.DMA((steps, 3)),
        ],
        name="gated",
    )(mine, theirs, far)


def lowered(hidden, down, late, first, half):
    width = late.shape[0]
    ny, nz, rows, _ = down.shape
    pair = 2 * ny * rows

    def kernel(hidden_ref, down_ref, late_ref, out_ref, left, first_units, last_units, arrived):
        moves = [
            pltpu.make_async_copy(hidden_ref.at[pl.ds(first, half)], left, arrived.at[0]),
            pltpu.make_async_copy(late_ref, last_units, arrived.at[1]),
        ]
        groups = [pl.ds(0, nz // 4), pl.ds(nz // 4, nz - nz // 4)]
        for i, group in enumerate(groups):
            moves.append(
                pltpu.make_async_copy(
                    down_ref.at[:, group], first_units.at[:, group], arrived.at[2 + i]
                )
            )
        for move in moves:
            move.start()
        for move in moves[:3]:
            move.wait()
        for z in range(0, nz, 2):
            if z == nz // 4:
                moves[3].wait()
            blocks = [first_units[y, z + i] for i in range(2) for y in range(ny)]
            at = slice(z * ny * rows, z * ny * rows + pair)
            right = jnp.concatenate([jnp.concatenate(blocks, axis=0), last_units[at, :]], axis=1)
            out_ref[:, at] = lax.dot_general(
                left[...], right, (((1,), (1,)), ((), ())), preferred_element_type=jnp.float32
            ).astype(out_ref.dtype)

    return pl.pallas_call(
        kernel,
        out_shape=jax.ShapeDtypeStruct((half, width), jnp.bfloat16),
        in_specs=[IN_HBM] * 3,
        out_specs=IN_VMEM,
        scratch_shapes=[
            pltpu.VMEM((half, hidden.shape[1]), jnp.bfloat16),
            pltpu.VMEM(down.shape, jnp.bfloat16),
            pltpu.VMEM(late.shape, jnp.bfloat16),
            pltpu.SemaphoreType.DMA((4,)),
        ],
        name="lowered",
    )(hidden, down, late)


def on_device(
    queries,
    key_rows,
    values,
    doc_ids,
    sink_logits,
    residual,
    out_weight,
    norm_gain,
    w_gate,
    w_up,
    w_down,
):
    rows, width = residual.shape
    half, share = rows // 2, rows // (2 * NX)
    core = lax.rem(lax.axis_index("tp"), 2)
    chip = lax.div(lax.axis_index("tp"), 2)
    ff = w_gate.shape[1]

    turned = w_down.T
    near = copies(jnp.concatenate([w_gate, w_up, turned[:, EARLY:]], axis=1), "sp", FAR_Y)
    near = near.reshape(-1, near.shape[2])
    far = lax.all_gather(near, "sp", axis=0, tiled=True, axis_index_groups=FAR_Z)

    attended = attend(queries, key_rows, values, doc_ids, sink_logits)
    at_mine = lax.dynamic_slice_in_dim(attended, core * half, half, 0)
    at_theirs = lax.dynamic_slice_in_dim(attended, (1 - core) * half, half, 0)
    pair_sum = pair_sum_of(
        jnp.dot(at_theirs, out_weight, preferred_element_type=jnp.float32).astype(jnp.bfloat16),
        jnp.dot(at_mine, out_weight, preferred_element_type=jnp.float32),
    )
    pieces = to_owners(pair_sum)
    early, _ = lax.optimization_barrier((turned[:, :EARLY], pair_sum))
    column = lax.all_gather(early, "sp", axis=0, tiled=True, axis_index_groups=FAR_Z)
    spread = jnp.broadcast_to(column[None], (NY, *column.shape))
    spread, pieces = lax.optimization_barrier((spread, pieces))
    down = swapped(spread, "sp", FAR_Y)
    down = down.reshape(NY, NZ, -1, EARLY)
    mixed_sum = pieces.astype(jnp.float32).sum(axis=0)
    base_rows = lax.dynamic_slice_in_dim(residual, core * half + chip * share, share, 0)
    stream = (base_rows.astype(jnp.float32) + mixed_sum).astype(jnp.bfloat16)
    normed = rms_norm(stream, norm_gain).astype(jnp.bfloat16)
    normed = all_chips_rows(normed, chip, pair_sum)
    theirs = other_core(normed)
    hidden, late = gated(normed, theirs, far, ff)

    pair_sum = pair_sum_of(
        lowered(hidden, down, late, half, half),
        lowered(hidden, down, late, 0, half).astype(jnp.float32),
    )
    mlp_total = to_owners(pair_sum).astype(jnp.float32).sum(axis=0)
    finished = (stream.astype(jnp.float32) + mlp_total).astype(jnp.bfloat16)
    mine = copies(finished, "tp", FAR_X).reshape(half, width)
    theirs = other_core(mine)
    whole = jnp.zeros((rows, width), jnp.bfloat16)
    whole = lax.dynamic_update_slice_in_dim(whole, mine, core * half, 0)
    return lax.dynamic_update_slice_in_dim(whole, theirs, (1 - core) * half, 0)


def solution(mesh):
    in_specs = (
        P("sp", "tp"),
        P("sp", "tp"),
        P("sp", "tp"),
        P("sp"),
        P("tp"),
        P("sp", None),
        P("tp", None),
        P(),
        P("sp", "tp"),
        P("sp", "tp"),
        P("tp", "sp"),
    )
    out_specs = P("sp", None)
    return jax.shard_map(
        on_device, mesh=mesh, in_specs=in_specs, out_specs=out_specs, check_vma=False
    )
```

```python
import jax
import jax.numpy as jnp
from jax import lax
from jax.sharding import PartitionSpec as P


HD = 64
WINDOW = 128
NZ, NY, NX = 16, 4, 4
EARLY = 512
FAR_Z = [[z * NY + y for z in range(NZ)] for y in range(NY)]
FAR_Y = [[z * NY + y for y in range(NY)] for z in range(NZ)]
FAR_X = [[2 * x + c for x in range(NX)] for c in range(2)]


def from_behind(shard, axis, by):
    size = lax.axis_size(axis)
    pairs = [(i, i + by) for i in range(size) if 0 <= i + by < size]
    return lax.ppermute(shard, axis, pairs)


def other_core(shard):
    return lax.ppermute(shard, "tp", [(i, i ^ 1) for i in range(2 * NX)])


def swapped(pieces, axis, groups):
    return lax.all_to_all(pieces, axis, 0, 0, tiled=True, axis_index_groups=groups)


def copies(shard, axis, groups):
    return swapped(jnp.broadcast_to(shard[None], (len(groups[0]), *shard.shape)), axis, groups)


def chip_away(shard, by):
    pairs = [(2 * x + c, 2 * ((x + by) % NX) + c) for x in range(NX) for c in range(2)]
    return lax.ppermute(shard, "tp", pairs)


def all_chips_rows(shard, chip):
    share = shard.shape[0]
    rows = jnp.zeros((NX * share, shard.shape[1]), shard.dtype)
    rows = lax.dynamic_update_slice_in_dim(rows, shard, chip * share, 0)
    for by in (1, 3, 2):
        sender = lax.rem(chip - by + NX, NX)
        rows = lax.dynamic_update_slice_in_dim(rows, chip_away(shard, by), sender * share, 0)
    return rows


def rms_norm(stream, norm_gain):
    floats = stream.astype(jnp.float32)
    scale = lax.rsqrt(jnp.mean(floats * floats, axis=-1, keepdims=True) + 1e-06)
    return floats * scale * norm_gain


def band_rows(tensor, blocks):
    tensor = tensor.reshape((blocks + 1, WINDOW) + tensor.shape[1:])
    return jnp.concatenate([tensor[:-1], tensor[1:]], axis=1)


def attend(queries, key_rows, values, doc_ids, sink_logits):
    local_rows = queries.shape[0]
    blocks = local_rows // WINDOW
    kv_local = key_rows.shape[1] // HD
    per_kv = queries.shape[1] // key_rows.shape[1]
    width = key_rows.shape[1]
    tail = local_rows - WINDOW
    tail_docs = (doc_ids[tail:] + 1).astype(jnp.bfloat16)
    tail_rows = jnp.concatenate([key_rows[tail:], values[tail:]], axis=1)
    docs_rows = jnp.broadcast_to(tail_docs.reshape(-1, 2 * width), (8 * WINDOW // (2 * width), 2 * width))
    before = from_behind(jnp.concatenate([tail_rows, docs_rows], axis=0), "sp", 1)
    prev_keys, prev_values = before[:WINDOW, :width], before[:WINDOW, width:]
    prev_docs = before[WINDOW].reshape(-1).astype(jnp.int32) - 1
    key_band = band_rows(jnp.concatenate([prev_keys, key_rows], axis=0), blocks).reshape(
        blocks, 2 * WINDOW, kv_local, HD
    )
    value_band = band_rows(jnp.concatenate([prev_values, values], axis=0), blocks).reshape(
        blocks, 2 * WINDOW, kv_local, HD
    )
    doc_band = band_rows(jnp.concatenate([prev_docs, doc_ids]), blocks)
    query_band = queries.reshape(blocks, WINDOW, kv_local, per_kv, HD)
    scores = jnp.einsum(
        "nqhgd,nkhd->nhgqk", query_band, key_band, preferred_element_type=jnp.float32
    ) * HD ** (-0.5)
    offsets = jnp.arange(WINDOW)[:, None] + WINDOW - jnp.arange(2 * WINDOW)[None, :]
    inside = (offsets >= 0) & (offsets < WINDOW)
    query_docs = doc_ids.reshape(blocks, WINDOW)
    allowed = inside[None] & (query_docs[:, :, None] == doc_band[:, None, :])
    scores = jnp.where(allowed[:, None, None], scores, -1e30)
    sink_logit = sink_logits.reshape(kv_local, per_kv)[None, :, :, None, None]
    peak = jnp.maximum(jnp.max(scores, axis=-1, keepdims=True), sink_logit)
    raised = jnp.exp(scores - peak)
    denom = jnp.sum(raised, axis=-1, keepdims=True) + jnp.exp(sink_logit - peak)
    weights = (raised / denom).astype(jnp.bfloat16)
    attended = jnp.einsum(
        "nhgqk,nkhd->nqhgd", weights, value_band, preferred_element_type=jnp.float32
    )
    return attended.astype(jnp.bfloat16).reshape(local_rows, queries.shape[1])


def side_by_side(arrays):
    whole = sum(a.shape[1] for a in arrays)
    low = jnp.array(-jnp.inf, arrays[0].dtype)
    at, joined = 0, None
    for a in arrays:
        padded = lax.pad(a, low, ((0, 0, 0), (at, whole - at - a.shape[1], 0)))
        joined = padded if joined is None else jnp.maximum(joined, padded)
        at += a.shape[1]
    return joined


def pair_sum_of(theirs, mine):
    arrived = other_core(theirs)
    return (mine + arrived.astype(jnp.float32)).astype(jnp.bfloat16)


def to_owners(pair_sum):
    return swapped(pair_sum.reshape(NX, -1, pair_sum.shape[1]), "tp", FAR_X)


def on_device(
    queries,
    key_rows,
    values,
    doc_ids,
    sink_logits,
    residual,
    out_weight,
    norm_gain,
    w_gate,
    w_up,
    w_down,
):
    rows, width = residual.shape
    half, share = rows // 2, rows // (2 * NX)
    core = lax.rem(lax.axis_index("tp"), 2)
    chip = lax.div(lax.axis_index("tp"), 2)
    ff = w_gate.shape[1]

    turned = w_down.T
    near = copies(side_by_side([w_gate, w_up, turned[:, EARLY:]]), "sp", FAR_Y)
    near = near.reshape(-1, near.shape[2])
    far = lax.all_gather(near, "sp", axis=0, tiled=True, axis_index_groups=FAR_Z)

    attended = attend(queries, key_rows, values, doc_ids, sink_logits)
    mixed = jnp.dot(attended, out_weight, preferred_element_type=jnp.float32).astype(jnp.bfloat16)
    pieces = lax.all_to_all(mixed.reshape(2 * NX, share, width), "tp", 0, 0, tiled=True)
    early, _ = lax.optimization_barrier((turned[:, :EARLY], mixed))
    column = lax.all_gather(early, "sp", axis=0, tiled=True, axis_index_groups=FAR_Z)
    spread = jnp.broadcast_to(column[None], (NY, *column.shape))
    spread, pieces = lax.optimization_barrier((spread, pieces))
    down = swapped(spread, "sp", FAR_Y)
    down = jnp.swapaxes(down.reshape(NY, NZ, -1, EARLY), 0, 1).reshape(width, EARLY)
    mixed_sum = pieces.astype(jnp.float32).sum(axis=0)
    base_rows = lax.dynamic_slice_in_dim(residual, lax.axis_index("tp") * share, share, 0)
    stream = (base_rows.astype(jnp.float32) + mixed_sum).astype(jnp.bfloat16)
    normed = rms_norm(stream, norm_gain).astype(jnp.bfloat16)
    normed = all_chips_rows(normed, chip)
    normed = jnp.concatenate([normed, other_core(normed)], axis=0)

    acts = jnp.dot(normed, far[:, : 2 * ff], preferred_element_type=jnp.float32)
    hidden = (jax.nn.silu(acts[:, :ff]) * acts[:, ff:]).astype(jnp.bfloat16)

    def turned_dot(left, right):
        return lax.dot_general(
            left, right, (((1,), (1,)), ((), ())), preferred_element_type=jnp.float32
        )

    late = far[:, 2 * ff :]

    def through(part):
        return turned_dot(part[:, EARLY:], late) + turned_dot(part[:, :EARLY], down)

    pair_sum = pair_sum_of(through(hidden[half:]).astype(jnp.bfloat16), through(hidden[:half]))
    mlp_total = to_owners(pair_sum).astype(jnp.float32).sum(axis=0)
    finished = (stream.astype(jnp.float32) + mlp_total).astype(jnp.bfloat16)
    mine = copies(finished, "tp", FAR_X).reshape(half, width)
    theirs = other_core(mine)
    whole = jnp.zeros((NX, 2, share, width), jnp.bfloat16)
    for part, at in ((mine, core), (theirs, 1 - core)):
        whole = lax.dynamic_update_slice_in_dim(whole, part.reshape(NX, 1, share, width), at, 1)
    return whole.reshape(rows, width)


def solution(mesh):
    in_specs = (
        P("sp", "tp"),
        P("sp", "tp"),
        P("sp", "tp"),
        P("sp"),
        P("tp"),
        P("sp", None),
        P("tp", None),
        P(),
        P("sp", "tp"),
        P("sp", "tp"),
        P("tp", "sp"),
    )
    out_specs = P("sp", None)
    return jax.shard_map(
        on_device, mesh=mesh, in_specs=in_specs, out_specs=out_specs, check_vma=False
    )
```

```python
import jax
import jax.numpy as jnp
from jax import lax
from jax.sharding import PartitionSpec as P


HD = 64
WINDOW = 128
NZ, NY, NX = 16, 4, 4
EARLY = 512
FAR_Z = [[z * NY + y for z in range(NZ)] for y in range(NY)]
FAR_Y = [[z * NY + y for y in range(NY)] for z in range(NZ)]
FAR_X = [[2 * x + c for x in range(NX)] for c in range(2)]


def from_behind(shard, axis, by):
    size = lax.axis_size(axis)
    pairs = [(i, i + by) for i in range(size) if 0 <= i + by < size]
    return lax.ppermute(shard, axis, pairs)


def other_core(shard):
    return lax.ppermute(shard, "tp", [(i, i ^ 1) for i in range(2 * NX)])


def swapped(pieces, axis, groups):
    return lax.all_to_all(pieces, axis, 0, 0, tiled=True, axis_index_groups=groups)


def copies(shard, axis, groups):
    return swapped(jnp.broadcast_to(shard[None], (len(groups[0]), *shard.shape)), axis, groups)


def chip_away(shard, by):
    pairs = [(2 * x + c, 2 * ((x + by) % NX) + c) for x in range(NX) for c in range(2)]
    return lax.ppermute(shard, "tp", pairs)


def all_chips_rows(shard, chip):
    share = shard.shape[0]
    rows = jnp.zeros((NX * share, shard.shape[1]), shard.dtype)
    rows = lax.dynamic_update_slice_in_dim(rows, shard, chip * share, 0)
    for by in (1, 3, 2):
        sender = lax.rem(chip - by + NX, NX)
        rows = lax.dynamic_update_slice_in_dim(rows, chip_away(shard, by), sender * share, 0)
    return rows


def rms_norm(stream, norm_gain):
    floats = stream.astype(jnp.float32)
    scale = lax.rsqrt(jnp.mean(floats * floats, axis=-1, keepdims=True) + 1e-06)
    return floats * scale * norm_gain


def band_rows(tensor, blocks):
    tensor = tensor.reshape((blocks + 1, WINDOW) + tensor.shape[1:])
    return jnp.concatenate([tensor[:-1], tensor[1:]], axis=1)


def attend(queries, key_rows, values, doc_ids, sink_logits):
    local_rows = queries.shape[0]
    blocks = local_rows // WINDOW
    kv_local = key_rows.shape[1] // HD
    per_kv = queries.shape[1] // key_rows.shape[1]
    width = key_rows.shape[1]
    tail = local_rows - WINDOW
    tail_docs = (doc_ids[tail:] + 1).astype(jnp.bfloat16)
    tail_rows = jnp.concatenate([key_rows[tail:], values[tail:]], axis=1)
    docs_rows = jnp.broadcast_to(tail_docs.reshape(-1, 2 * width), (8 * WINDOW // (2 * width), 2 * width))
    before = from_behind(jnp.concatenate([tail_rows, docs_rows], axis=0), "sp", 1)
    prev_keys, prev_values = before[:WINDOW, :width], before[:WINDOW, width:]
    prev_docs = before[WINDOW].reshape(-1).astype(jnp.int32) - 1
    key_band = band_rows(jnp.concatenate([prev_keys, key_rows], axis=0), blocks).reshape(
        blocks, 2 * WINDOW, kv_local, HD
    )
    value_band = band_rows(jnp.concatenate([prev_values, values], axis=0), blocks).reshape(
        blocks, 2 * WINDOW, kv_local, HD
    )
    doc_band = band_rows(jnp.concatenate([prev_docs, doc_ids]), blocks)
    query_band = queries.reshape(blocks, WINDOW, kv_local, per_kv, HD)
    scores = jnp.einsum(
        "nqhgd,nkhd->nhgqk", query_band, key_band, preferred_element_type=jnp.float32
    ) * HD ** (-0.5)
    offsets = jnp.arange(WINDOW)[:, None] + WINDOW - jnp.arange(2 * WINDOW)[None, :]
    inside = (offsets >= 0) & (offsets < WINDOW)
    query_docs = doc_ids.reshape(blocks, WINDOW)
    allowed = inside[None] & (query_docs[:, :, None] == doc_band[:, None, :])
    scores = jnp.where(allowed[:, None, None], scores, -1e30)
    sink_logit = sink_logits.reshape(kv_local, per_kv)[None, :, :, None, None]
    peak = jnp.maximum(jnp.max(scores, axis=-1, keepdims=True), sink_logit)
    raised = jnp.exp(scores - peak)
    denom = jnp.sum(raised, axis=-1, keepdims=True) + jnp.exp(sink_logit - peak)
    weights = (raised / denom).astype(jnp.bfloat16)
    attended = jnp.einsum(
        "nhgqk,nkhd->nqhgd", weights, value_band, preferred_element_type=jnp.float32
    )
    return attended.astype(jnp.bfloat16).reshape(local_rows, queries.shape[1])


def side_by_side(w_gate, w_up, turned):
    ff = w_gate.shape[1]
    whole = 3 * ff - EARLY
    zero = jnp.zeros((), w_gate.dtype)
    column = lax.broadcasted_iota(jnp.int32, (w_gate.shape[0], whole), 1)

    def placed(array, at):
        return lax.pad(array, zero, ((0, 0, 0), (at, whole - at - ff, 0)))

    last = placed(turned, whole - ff)
    return jnp.where(
        column < ff, placed(w_gate, 0), jnp.where(column < 2 * ff, placed(w_up, ff), last)
    )


def pair_sum_of(theirs, mine):
    arrived = other_core(theirs)
    return (mine + arrived.astype(jnp.float32)).astype(jnp.bfloat16)


def to_owners(pair_sum):
    return swapped(pair_sum.reshape(NX, -1, pair_sum.shape[1]), "tp", FAR_X)


def on_device(
    queries,
    key_rows,
    values,
    doc_ids,
    sink_logits,
    residual,
    out_weight,
    norm_gain,
    w_gate,
    w_up,
    w_down,
):
    rows, width = residual.shape
    half, share = rows // 2, rows // (2 * NX)
    core = lax.rem(lax.axis_index("tp"), 2)
    chip = lax.div(lax.axis_index("tp"), 2)
    ff = w_gate.shape[1]

    turned = w_down.T
    near = copies(side_by_side(w_gate, w_up, turned), "sp", FAR_Y)
    near = near.reshape(-1, near.shape[2])
    far = lax.all_gather(near, "sp", axis=0, tiled=True, axis_index_groups=FAR_Z)

    attended = attend(queries, key_rows, values, doc_ids, sink_logits)
    attended = jnp.swapaxes(attended.reshape(2, NX, share, -1), 0, 1).reshape(rows, -1)
    mixed = jnp.dot(attended, out_weight, preferred_element_type=jnp.float32).astype(jnp.bfloat16)
    pieces = lax.all_to_all(mixed.reshape(2 * NX, share, width), "tp", 0, 0, tiled=True)
    early, _ = lax.optimization_barrier((turned[:, :EARLY], mixed))
    column = lax.all_gather(early, "sp", axis=0, tiled=True, axis_index_groups=FAR_Z)
    spread = jnp.broadcast_to(column[None], (NY, *column.shape))
    spread, pieces = lax.optimization_barrier((spread, pieces))
    down = swapped(spread, "sp", FAR_Y)
    down = jnp.swapaxes(down.reshape(NY, NZ, -1, EARLY), 0, 1).reshape(width, EARLY)
    mixed_sum = pieces.astype(jnp.float32).sum(axis=0)
    base_rows = lax.dynamic_slice_in_dim(residual, core * half + chip * share, share, 0)
    stream = (base_rows.astype(jnp.float32) + mixed_sum).astype(jnp.bfloat16)
    normed = rms_norm(stream, norm_gain).astype(jnp.bfloat16)
    normed = all_chips_rows(normed, chip)
    normed = jnp.concatenate([normed, other_core(normed)], axis=0)

    late = far[:, 2 * ff :]
    acts = jnp.dot(normed, far[:, : 2 * ff], preferred_element_type=jnp.float32)
    hidden = (jax.nn.silu(acts[:, :ff]) * acts[:, ff:]).astype(jnp.bfloat16)

    def turned_dot(left, right):
        return lax.dot_general(
            left, right, (((1,), (1,)), ((), ())), preferred_element_type=jnp.float32
        )


    def through(part):
        return turned_dot(part[:, EARLY:], late) + turned_dot(part[:, :EARLY], down)

    pair_sum = pair_sum_of(through(hidden[half:]).astype(jnp.bfloat16), through(hidden[:half]))
    mlp_total = to_owners(pair_sum).astype(jnp.float32).sum(axis=0)
    finished = (stream.astype(jnp.float32) + mlp_total).astype(jnp.bfloat16)
    mine = copies(finished, "tp", FAR_X).reshape(half, width)
    theirs = other_core(mine)
    whole = jnp.zeros((rows, width), jnp.bfloat16)
    whole = lax.dynamic_update_slice_in_dim(whole, mine, core * half, 0)
    return lax.dynamic_update_slice_in_dim(whole, theirs, (1 - core) * half, 0)


def solution(mesh):
    in_specs = (
        P("sp", "tp"),
        P("sp", "tp"),
        P("sp", "tp"),
        P("sp"),
        P("tp"),
        P("sp", None),
        P("tp", None),
        P(),
        P("sp", "tp"),
        P("sp", "tp"),
        P("tp", "sp"),
    )
    out_specs = P("sp", None)
    return jax.shard_map(
        on_device, mesh=mesh, in_specs=in_specs, out_specs=out_specs, check_vma=False
    )
```

```python
import jax
import jax.numpy as jnp
from jax import lax
from jax.sharding import PartitionSpec as P


HD = 64
WINDOW = 128
NZ, NY, NX = 16, 4, 4
EARLY = 512
FAR_Z = [[z * NY + y for z in range(NZ)] for y in range(NY)]
FAR_Y = [[z * NY + y for y in range(NY)] for z in range(NZ)]
FAR_X = [[2 * x + c for x in range(NX)] for c in range(2)]


def from_behind(shard, axis, by):
    size = lax.axis_size(axis)
    pairs = [(i, i + by) for i in range(size) if 0 <= i + by < size]
    return lax.ppermute(shard, axis, pairs)


def other_core(shard):
    return lax.ppermute(shard, "tp", [(i, i ^ 1) for i in range(2 * NX)])


def swapped(pieces, axis, groups):
    return lax.all_to_all(pieces, axis, 0, 0, tiled=True, axis_index_groups=groups)


def copies(shard, axis, groups):
    return swapped(jnp.broadcast_to(shard[None], (len(groups[0]), *shard.shape)), axis, groups)


def chip_away(shard, by):
    pairs = [(2 * x + c, 2 * ((x + by) % NX) + c) for x in range(NX) for c in range(2)]
    return lax.ppermute(shard, "tp", pairs)


def all_chips_rows(shard, chip):
    share = shard.shape[0]
    rows = jnp.zeros((NX * share, shard.shape[1]), shard.dtype)
    rows = lax.dynamic_update_slice_in_dim(rows, shard, chip * share, 0)
    for by in (1, 3, 2):
        sender = lax.rem(chip - by + NX, NX)
        rows = lax.dynamic_update_slice_in_dim(rows, chip_away(shard, by), sender * share, 0)
    return rows


def rms_norm(stream, norm_gain):
    floats = stream.astype(jnp.float32)
    scale = lax.rsqrt(jnp.mean(floats * floats, axis=-1, keepdims=True) + 1e-06)
    return floats * scale * norm_gain


def band_rows(tensor, blocks):
    tensor = tensor.reshape((blocks + 1, WINDOW) + tensor.shape[1:])
    return jnp.concatenate([tensor[:-1], tensor[1:]], axis=1)


def attend(queries, key_rows, values, doc_ids, sink_logits):
    local_rows = queries.shape[0]
    blocks = local_rows // WINDOW
    kv_local = key_rows.shape[1] // HD
    per_kv = queries.shape[1] // key_rows.shape[1]
    width = key_rows.shape[1]
    tail = local_rows - WINDOW
    tail_docs = (doc_ids[tail:] + 1).astype(jnp.bfloat16)
    tail_rows = jnp.concatenate([key_rows[tail:], values[tail:]], axis=1)
    docs_rows = jnp.broadcast_to(tail_docs.reshape(-1, 2 * width), (8 * WINDOW // (2 * width), 2 * width))
    before = from_behind(jnp.concatenate([tail_rows, docs_rows], axis=0), "sp", 1)
    prev_keys, prev_values = before[:WINDOW, :width], before[:WINDOW, width:]
    prev_docs = before[WINDOW].reshape(-1).astype(jnp.int32) - 1
    key_band = band_rows(jnp.concatenate([prev_keys, key_rows], axis=0), blocks).reshape(
        blocks, 2 * WINDOW, kv_local, HD
    )
    value_band = band_rows(jnp.concatenate([prev_values, values], axis=0), blocks).reshape(
        blocks, 2 * WINDOW, kv_local, HD
    )
    doc_band = band_rows(jnp.concatenate([prev_docs, doc_ids]), blocks)
    query_band = queries.reshape(blocks, WINDOW, kv_local, per_kv, HD)
    scores = jnp.einsum(
        "nqhgd,nkhd->nhgqk", query_band, key_band, preferred_element_type=jnp.float32
    ) * HD ** (-0.5)
    offsets = jnp.arange(WINDOW)[:, None] + WINDOW - jnp.arange(2 * WINDOW)[None, :]
    inside = (offsets >= 0) & (offsets < WINDOW)
    query_docs = doc_ids.reshape(blocks, WINDOW)
    allowed = inside[None] & (query_docs[:, :, None] == doc_band[:, None, :])
    scores = jnp.where(allowed[:, None, None], scores, -1e30)
    sink_logit = sink_logits.reshape(kv_local, per_kv)[None, :, :, None, None]
    peak = jnp.maximum(jnp.max(scores, axis=-1, keepdims=True), sink_logit)
    raised = jnp.exp(scores - peak)
    denom = jnp.sum(raised, axis=-1, keepdims=True) + jnp.exp(sink_logit - peak)
    weights = (raised / denom).astype(jnp.bfloat16)
    attended = jnp.einsum(
        "nhgqk,nkhd->nqhgd", weights, value_band, preferred_element_type=jnp.float32
    )
    return attended.astype(jnp.bfloat16).reshape(local_rows, queries.shape[1])


def side_by_side(w_gate, w_up, turned):
    ff = w_gate.shape[1]
    whole = 3 * ff - EARLY
    zero = jnp.zeros((), w_gate.dtype)
    column = lax.broadcasted_iota(jnp.int32, (w_gate.shape[0], whole), 1)

    def placed(array, at):
        return lax.pad(array, zero, ((0, 0, 0), (at, whole - at - ff, 0)))

    last = placed(turned, whole - ff)
    return jnp.where(
        column < ff, placed(w_gate, 0), jnp.where(column < 2 * ff, placed(w_up, ff), last)
    )


def to_owners(pair_sum):
    return swapped(pair_sum.reshape(NX, -1, pair_sum.shape[1]), "tp", FAR_X)


def on_device(
    queries,
    key_rows,
    values,
    doc_ids,
    sink_logits,
    residual,
    out_weight,
    norm_gain,
    w_gate,
    w_up,
    w_down,
):
    rows, width = residual.shape
    half, share = rows // 2, rows // (2 * NX)
    core = lax.rem(lax.axis_index("tp"), 2)
    chip = lax.div(lax.axis_index("tp"), 2)
    ff = w_gate.shape[1]

    turned = w_down.T
    near = lax.all_gather(
        side_by_side(w_gate, w_up, turned), "sp", axis=0, tiled=True, axis_index_groups=FAR_Y
    )
    far = lax.all_gather(near, "sp", axis=0, tiled=True, axis_index_groups=FAR_Z)

    attended = attend(queries, key_rows, values, doc_ids, sink_logits)
    attended = jnp.swapaxes(attended.reshape(2, NX, share, -1), 0, 1).reshape(rows, -1)
    mixed = jnp.dot(attended, out_weight, preferred_element_type=jnp.float32).astype(jnp.bfloat16)
    pieces = lax.all_to_all(mixed.reshape(2 * NX, share, width), "tp", 0, 0, tiled=True)
    early, _ = lax.optimization_barrier((turned[:, :EARLY], mixed))
    column = lax.all_gather(early, "sp", axis=0, tiled=True, axis_index_groups=FAR_Z)
    spread = jnp.broadcast_to(column[None], (NY, *column.shape))
    spread, pieces = lax.optimization_barrier((spread, pieces))
    down = swapped(spread, "sp", FAR_Y)
    down = jnp.swapaxes(down.reshape(NY, NZ, -1, EARLY), 0, 1).reshape(width, EARLY)
    mixed_sum = pieces.astype(jnp.float32).sum(axis=0)
    base_rows = lax.dynamic_slice_in_dim(residual, core * half + chip * share, share, 0)
    stream = (base_rows.astype(jnp.float32) + mixed_sum).astype(jnp.bfloat16)
    normed = rms_norm(stream, norm_gain).astype(jnp.bfloat16)
    normed = all_chips_rows(normed, chip)
    normed = jnp.concatenate([normed, other_core(normed)], axis=0)
    normed, far, down = lax.optimization_barrier((normed, far, down))

    late = far[:, 2 * ff :]
    acts = jnp.dot(normed, far[:, : 2 * ff], preferred_element_type=jnp.float32)
    hidden = (jax.nn.silu(acts[:, :ff]) * acts[:, ff:]).astype(jnp.bfloat16)

    def turned_dot(left, right):
        return lax.dot_general(
            left, right, (((1,), (1,)), ((), ())), preferred_element_type=jnp.float32
        )


    def through(part):
        return turned_dot(part[:, EARLY:], late) + turned_dot(part[:, :EARLY], down)

    swapped_part = other_core(through(hidden[half:]).astype(jnp.bfloat16))
    own_part, swapped_part = lax.optimization_barrier((through(hidden[:half]), swapped_part))
    pair_sum = (own_part + swapped_part.astype(jnp.float32)).astype(jnp.bfloat16)
    mlp_total = to_owners(pair_sum).astype(jnp.float32).sum(axis=0)
    finished = (stream.astype(jnp.float32) + mlp_total).astype(jnp.bfloat16)
    mine = copies(finished, "tp", FAR_X).reshape(half, width)
    theirs = other_core(mine)
    whole = jnp.zeros((rows, width), jnp.bfloat16)
    whole = lax.dynamic_update_slice_in_dim(whole, mine, core * half, 0)
    return lax.dynamic_update_slice_in_dim(whole, theirs, (1 - core) * half, 0)


def solution(mesh):
    in_specs = (
        P("sp", "tp"),
        P("sp", "tp"),
        P("sp", "tp"),
        P("sp"),
        P("tp"),
        P("sp", None),
        P("tp", None),
        P(),
        P("sp", "tp"),
        P("sp", "tp"),
        P("tp", "sp"),
    )
    out_specs = P("sp", None)
    return jax.shard_map(
        on_device, mesh=mesh, in_specs=in_specs, out_specs=out_specs, check_vma=False
    )
```

```python
import jax
import jax.numpy as jnp
from jax import lax
from jax.sharding import PartitionSpec as P


HD = 64
WINDOW = 128
NZ, NY, NX = 16, 4, 4
EARLY = 512
FAR_Z = [[z * NY + y for z in range(NZ)] for y in range(NY)]
FAR_Y = [[z * NY + y for y in range(NY)] for z in range(NZ)]
FAR_X = [[2 * x + c for x in range(NX)] for c in range(2)]


def from_behind(shard, axis, by):
    size = lax.axis_size(axis)
    pairs = [(i, i + by) for i in range(size) if 0 <= i + by < size]
    return lax.ppermute(shard, axis, pairs)


def other_core(shard):
    return lax.ppermute(shard, "tp", [(i, i ^ 1) for i in range(2 * NX)])


def swapped(pieces, axis, groups):
    return lax.all_to_all(pieces, axis, 0, 0, tiled=True, axis_index_groups=groups)


def copies(shard, axis, groups):
    return swapped(jnp.broadcast_to(shard[None], (len(groups[0]), *shard.shape)), axis, groups)


def chip_away(shard, by):
    pairs = [(2 * x + c, 2 * ((x + by) % NX) + c) for x in range(NX) for c in range(2)]
    return lax.ppermute(shard, "tp", pairs)


def all_chips_rows(shard, chip):
    share = shard.shape[0]
    rows = jnp.zeros((NX * share, shard.shape[1]), shard.dtype)
    rows = lax.dynamic_update_slice_in_dim(rows, shard, chip * share, 0)
    for by in (1, 3, 2):
        sender = lax.rem(chip - by + NX, NX)
        rows = lax.dynamic_update_slice_in_dim(rows, chip_away(shard, by), sender * share, 0)
    return rows


def rms_norm(stream, norm_gain):
    floats = stream.astype(jnp.float32)
    scale = lax.rsqrt(jnp.mean(floats * floats, axis=-1, keepdims=True) + 1e-06)
    return floats * scale * norm_gain


def band_rows(tensor, blocks):
    tensor = tensor.reshape((blocks + 1, WINDOW) + tensor.shape[1:])
    return jnp.concatenate([tensor[:-1], tensor[1:]], axis=1)


def attend(queries, key_rows, values, doc_ids, sink_logits):
    local_rows = queries.shape[0]
    blocks = local_rows // WINDOW
    kv_local = key_rows.shape[1] // HD
    per_kv = queries.shape[1] // key_rows.shape[1]
    width = key_rows.shape[1]
    tail = local_rows - WINDOW
    tail_docs = (doc_ids[tail:] + 1).astype(jnp.bfloat16)
    tail_rows = jnp.concatenate([key_rows[tail:], values[tail:]], axis=1)
    docs_rows = jnp.broadcast_to(tail_docs.reshape(-1, 2 * width), (8 * WINDOW // (2 * width), 2 * width))
    before = from_behind(jnp.concatenate([tail_rows, docs_rows], axis=0), "sp", 1)
    prev_keys, prev_values = before[:WINDOW, :width], before[:WINDOW, width:]
    prev_docs = before[WINDOW].reshape(-1).astype(jnp.int32) - 1
    key_band = band_rows(jnp.concatenate([prev_keys, key_rows], axis=0), blocks).reshape(
        blocks, 2 * WINDOW, kv_local, HD
    )
    value_band = band_rows(jnp.concatenate([prev_values, values], axis=0), blocks).reshape(
        blocks, 2 * WINDOW, kv_local, HD
    )
    doc_band = band_rows(jnp.concatenate([prev_docs, doc_ids]), blocks)
    query_band = queries.reshape(blocks, WINDOW, kv_local, per_kv, HD)
    scores = jnp.einsum(
        "nqhgd,nkhd->nhgqk", query_band, key_band, preferred_element_type=jnp.float32
    ) * HD ** (-0.5)
    offsets = jnp.arange(WINDOW)[:, None] + WINDOW - jnp.arange(2 * WINDOW)[None, :]
    inside = (offsets >= 0) & (offsets < WINDOW)
    query_docs = doc_ids.reshape(blocks, WINDOW)
    allowed = inside[None] & (query_docs[:, :, None] == doc_band[:, None, :])
    scores = jnp.where(allowed[:, None, None], scores, -1e30)
    sink_logit = sink_logits.reshape(kv_local, per_kv)[None, :, :, None, None]
    peak = jnp.maximum(jnp.max(scores, axis=-1, keepdims=True), sink_logit)
    raised = jnp.exp(scores - peak)
    denom = jnp.sum(raised, axis=-1, keepdims=True) + jnp.exp(sink_logit - peak)
    weights = (raised / denom).astype(jnp.bfloat16)
    attended = jnp.einsum(
        "nhgqk,nkhd->nqhgd", weights, value_band, preferred_element_type=jnp.float32
    )
    return attended.astype(jnp.bfloat16).reshape(local_rows, queries.shape[1])


def side_by_side(w_gate, w_up, turned):
    ff = w_gate.shape[1]
    whole = 3 * ff - EARLY
    zero = jnp.zeros((), w_gate.dtype)
    column = lax.broadcasted_iota(jnp.int32, (w_gate.shape[0], whole), 1)

    def placed(array, at):
        return lax.pad(array, zero, ((0, 0, 0), (at, whole - at - ff, 0)))

    last = placed(turned, whole - ff)
    return jnp.where(
        column < ff, placed(w_gate, 0), jnp.where(column < 2 * ff, placed(w_up, ff), last)
    )


def to_owners(pair_sum):
    return swapped(pair_sum.reshape(NX, -1, pair_sum.shape[1]), "tp", FAR_X)


def on_device(
    queries,
    key_rows,
    values,
    doc_ids,
    sink_logits,
    residual,
    out_weight,
    norm_gain,
    w_gate,
    w_up,
    w_down,
):
    rows, width = residual.shape
    half, share = rows // 2, rows // (2 * NX)
    core = lax.rem(lax.axis_index("tp"), 2)
    chip = lax.div(lax.axis_index("tp"), 2)
    ff = w_gate.shape[1]

    turned = w_down.T
    near = copies(side_by_side(w_gate, w_up, turned), "sp", FAR_Y)
    near = near.reshape(-1, near.shape[2])
    far = lax.all_gather(near, "sp", axis=0, tiled=True, axis_index_groups=FAR_Z)

    attended = attend(queries, key_rows, values, doc_ids, sink_logits)
    attended = jnp.swapaxes(attended.reshape(2, NX, share, -1), 0, 1).reshape(rows, -1)
    mixed = jnp.dot(attended, out_weight, preferred_element_type=jnp.float32).astype(jnp.bfloat16)
    pieces = lax.all_to_all(mixed.reshape(2 * NX, share, width), "tp", 0, 0, tiled=True)
    early, _ = lax.optimization_barrier((turned[:, :EARLY], mixed))
    column = lax.all_gather(early, "sp", axis=0, tiled=True, axis_index_groups=FAR_Z)
    spread = jnp.broadcast_to(column[None], (NY, *column.shape))
    spread, pieces = lax.optimization_barrier((spread, pieces))
    down = swapped(spread, "sp", FAR_Y)
    down = jnp.swapaxes(down.reshape(NY, NZ, -1, EARLY), 0, 1).reshape(width, EARLY)
    mixed_sum = pieces.astype(jnp.float32).sum(axis=0)
    base_rows = lax.dynamic_slice_in_dim(residual, core * half + chip * share, share, 0)
    stream = (base_rows.astype(jnp.float32) + mixed_sum).astype(jnp.bfloat16)
    normed = rms_norm(stream, norm_gain).astype(jnp.bfloat16)
    normed = all_chips_rows(normed, chip)
    normed = jnp.concatenate([normed, other_core(normed)], axis=0)
    normed, far, down = lax.optimization_barrier((normed, far, down))

    late = far[:, 2 * ff :]
    acts = lax.dot_general(
        far[:, : 2 * ff], normed, (((0,), (1,)), ((), ())), preferred_element_type=jnp.float32
    )
    hidden = (jax.nn.silu(acts[:ff]) * acts[ff:]).astype(jnp.bfloat16)

    def turned_dot(left, right):
        return lax.dot_general(
            left, right, (((0,), (1,)), ((), ())), preferred_element_type=jnp.float32
        )

    def through(part):
        return turned_dot(part[EARLY:], late) + turned_dot(part[:EARLY], down)

    swapped_part = other_core(through(hidden[:, half:]).astype(jnp.bfloat16))
    own_part, swapped_part = lax.optimization_barrier((through(hidden[:, :half]), swapped_part))
    pair_sum = (own_part + swapped_part.astype(jnp.float32)).astype(jnp.bfloat16)
    mlp_total = to_owners(pair_sum).astype(jnp.float32).sum(axis=0)
    finished = (stream.astype(jnp.float32) + mlp_total).astype(jnp.bfloat16)
    mine = copies(finished, "tp", FAR_X).reshape(half, width)
    theirs = other_core(mine)
    whole = jnp.zeros((rows, width), jnp.bfloat16)
    whole = lax.dynamic_update_slice_in_dim(whole, mine, core * half, 0)
    return lax.dynamic_update_slice_in_dim(whole, theirs, (1 - core) * half, 0)


def solution(mesh):
    in_specs = (
        P("sp", "tp"),
        P("sp", "tp"),
        P("sp", "tp"),
        P("sp"),
        P("tp"),
        P("sp", None),
        P("tp", None),
        P(),
        P("sp", "tp"),
        P("sp", "tp"),
        P("tp", "sp"),
    )
    out_specs = P("sp", None)
    return jax.shard_map(
        on_device, mesh=mesh, in_specs=in_specs, out_specs=out_specs, check_vma=False
    )
```

```python
import jax
import jax.numpy as jnp
from jax import lax
from jax.sharding import PartitionSpec as P


HD = 64
WINDOW = 128
NZ, NY, NX = 16, 4, 4
EARLY = 640
FAR_Z = [[z * NY + y for z in range(NZ)] for y in range(NY)]
FAR_Y = [[z * NY + y for y in range(NY)] for z in range(NZ)]
FAR_X = [[2 * x + c for x in range(NX)] for c in range(2)]


def from_behind(shard, axis, by):
    size = lax.axis_size(axis)
    pairs = [(i, i + by) for i in range(size) if 0 <= i + by < size]
    return lax.ppermute(shard, axis, pairs)


def other_core(shard):
    return lax.ppermute(shard, "tp", [(i, i ^ 1) for i in range(2 * NX)])


def swapped(pieces, axis, groups):
    return lax.all_to_all(pieces, axis, 0, 0, tiled=True, axis_index_groups=groups)


def copies(shard, axis, groups):
    return swapped(jnp.broadcast_to(shard[None], (len(groups[0]), *shard.shape)), axis, groups)


def chip_away(shard, by):
    pairs = [(2 * x + c, 2 * ((x + by) % NX) + c) for x in range(NX) for c in range(2)]
    return lax.ppermute(shard, "tp", pairs)


def all_chips_rows(shard, chip):
    share = shard.shape[0]
    rows = jnp.zeros((NX * share, shard.shape[1]), shard.dtype)
    rows = lax.dynamic_update_slice_in_dim(rows, shard, chip * share, 0)
    for by in (1, 3, 2):
        sender = lax.rem(chip - by + NX, NX)
        rows = lax.dynamic_update_slice_in_dim(rows, chip_away(shard, by), sender * share, 0)
    return rows


def rms_norm(stream, norm_gain):
    floats = stream.astype(jnp.float32)
    scale = lax.rsqrt(jnp.mean(floats * floats, axis=-1, keepdims=True) + 1e-06)
    return floats * scale * norm_gain


def band_rows(tensor, blocks):
    tensor = tensor.reshape((blocks + 1, WINDOW) + tensor.shape[1:])
    return jnp.concatenate([tensor[:-1], tensor[1:]], axis=1)


def attend(queries, key_rows, values, doc_ids, sink_logits):
    local_rows = queries.shape[0]
    blocks = local_rows // WINDOW
    kv_local = key_rows.shape[1] // HD
    per_kv = queries.shape[1] // key_rows.shape[1]
    width = key_rows.shape[1]
    tail = local_rows - WINDOW
    tail_docs = (doc_ids[tail:] + 1).astype(jnp.bfloat16)
    tail_rows = jnp.concatenate([key_rows[tail:], values[tail:]], axis=1)
    docs_rows = jnp.broadcast_to(tail_docs.reshape(-1, 2 * width), (8 * WINDOW // (2 * width), 2 * width))
    before = from_behind(jnp.concatenate([tail_rows, docs_rows], axis=0), "sp", 1)
    prev_keys, prev_values = before[:WINDOW, :width], before[:WINDOW, width:]
    prev_docs = before[WINDOW].reshape(-1).astype(jnp.int32) - 1
    key_band = band_rows(jnp.concatenate([prev_keys, key_rows], axis=0), blocks).reshape(
        blocks, 2 * WINDOW, kv_local, HD
    )
    value_band = band_rows(jnp.concatenate([prev_values, values], axis=0), blocks).reshape(
        blocks, 2 * WINDOW, kv_local, HD
    )
    doc_band = band_rows(jnp.concatenate([prev_docs, doc_ids]), blocks)
    query_band = queries.reshape(blocks, WINDOW, kv_local, per_kv, HD)
    scores = jnp.einsum(
        "nqhgd,nkhd->nhgqk", query_band, key_band, preferred_element_type=jnp.float32
    ) * HD ** (-0.5)
    offsets = jnp.arange(WINDOW)[:, None] + WINDOW - jnp.arange(2 * WINDOW)[None, :]
    inside = (offsets >= 0) & (offsets < WINDOW)
    query_docs = doc_ids.reshape(blocks, WINDOW)
    allowed = inside[None] & (query_docs[:, :, None] == doc_band[:, None, :])
    scores = jnp.where(allowed[:, None, None], scores, -1e30)
    sink_logit = sink_logits.reshape(kv_local, per_kv)[None, :, :, None, None]
    peak = jnp.maximum(jnp.max(scores, axis=-1, keepdims=True), sink_logit)
    raised = jnp.exp(scores - peak)
    denom = jnp.sum(raised, axis=-1, keepdims=True) + jnp.exp(sink_logit - peak)
    weights = (raised / denom).astype(jnp.bfloat16)
    attended = jnp.einsum(
        "nhgqk,nkhd->nqhgd", weights, value_band, preferred_element_type=jnp.float32
    )
    return attended.astype(jnp.bfloat16).reshape(local_rows, queries.shape[1])


def side_by_side(w_gate, w_up, turned):
    ff = w_gate.shape[1]
    whole = 3 * ff - EARLY
    zero = jnp.zeros((), w_gate.dtype)
    column = lax.broadcasted_iota(jnp.int32, (w_gate.shape[0], whole), 1)

    def placed(array, at):
        return lax.pad(array, zero, ((0, 0, 0), (at, whole - at - ff, 0)))

    last = placed(turned, whole - ff)
    return jnp.where(
        column < ff, placed(w_gate, 0), jnp.where(column < 2 * ff, placed(w_up, ff), last)
    )


def to_owners(pair_sum):
    return swapped(pair_sum.reshape(NX, -1, pair_sum.shape[1]), "tp", FAR_X)


def on_device(
    queries,
    key_rows,
    values,
    doc_ids,
    sink_logits,
    residual,
    out_weight,
    norm_gain,
    w_gate,
    w_up,
    w_down,
):
    rows, width = residual.shape
    half, share = rows // 2, rows // (2 * NX)
    core = lax.rem(lax.axis_index("tp"), 2)
    chip = lax.div(lax.axis_index("tp"), 2)
    ff = w_gate.shape[1]

    turned = w_down.T
    near = copies(side_by_side(w_gate, w_up, turned), "sp", FAR_Y)
    near = near.reshape(-1, near.shape[2])
    far = lax.all_gather(near, "sp", axis=0, tiled=True, axis_index_groups=FAR_Z)

    attended = attend(queries, key_rows, values, doc_ids, sink_logits)
    attended = jnp.swapaxes(attended.reshape(2, NX, share, -1), 0, 1).reshape(rows, -1)
    mixed = jnp.dot(attended, out_weight, preferred_element_type=jnp.float32).astype(jnp.bfloat16)
    pieces = lax.all_to_all(mixed.reshape(2 * NX, share, width), "tp", 0, 0, tiled=True)
    early, _ = lax.optimization_barrier((turned[:, :EARLY], mixed))
    column = lax.all_gather(early, "sp", axis=0, tiled=True, axis_index_groups=FAR_Z)
    spread = jnp.broadcast_to(column[None], (NY, *column.shape))
    spread, pieces = lax.optimization_barrier((spread, pieces))
    down = swapped(spread, "sp", FAR_Y)
    down = jnp.swapaxes(down.reshape(NY, NZ, -1, EARLY), 0, 1).reshape(width, EARLY)
    mixed_sum = pieces.astype(jnp.float32).sum(axis=0)
    base_rows = lax.dynamic_slice_in_dim(residual, core * half + chip * share, share, 0)
    stream = (base_rows.astype(jnp.float32) + mixed_sum).astype(jnp.bfloat16)
    normed = rms_norm(stream, norm_gain).astype(jnp.bfloat16)
    normed = all_chips_rows(normed, chip)
    normed = jnp.concatenate([normed, other_core(normed)], axis=0)
    normed, far = lax.optimization_barrier((normed, far))

    late = far[:, 2 * ff :]
    acts = jnp.dot(normed, far[:, : 2 * ff], preferred_element_type=jnp.float32)
    hidden = (jax.nn.silu(acts[:, :ff]) * acts[:, ff:]).astype(jnp.bfloat16)

    def turned_dot(left, right):
        return lax.dot_general(
            left, right, (((1,), (1,)), ((), ())), preferred_element_type=jnp.float32
        )


    def through(part):
        return turned_dot(part[:, EARLY:], late) + turned_dot(part[:, :EARLY], down)

    swapped_part = other_core(through(hidden[half:]).astype(jnp.bfloat16))
    own_part, swapped_part = lax.optimization_barrier((through(hidden[:half]), swapped_part))
    pair_sum = (own_part + swapped_part.astype(jnp.float32)).astype(jnp.bfloat16)
    mlp_total = to_owners(pair_sum).astype(jnp.float32).sum(axis=0)
    finished = (stream.astype(jnp.float32) + mlp_total).astype(jnp.bfloat16)
    mine = copies(finished, "tp", FAR_X).reshape(half, width)
    theirs = other_core(mine)
    whole = jnp.zeros((rows, width), jnp.bfloat16)
    whole = lax.dynamic_update_slice_in_dim(whole, mine, core * half, 0)
    return lax.dynamic_update_slice_in_dim(whole, theirs, (1 - core) * half, 0)


def solution(mesh):
    in_specs = (
        P("sp", "tp"),
        P("sp", "tp"),
        P("sp", "tp"),
        P("sp"),
        P("tp"),
        P("sp", None),
        P("tp", None),
        P(),
        P("sp", "tp"),
        P("sp", "tp"),
        P("tp", "sp"),
    )
    out_specs = P("sp", None)
    return jax.shard_map(
        on_device, mesh=mesh, in_specs=in_specs, out_specs=out_specs, check_vma=False
    )
```
